128 devices in a mesh: sp: 32 (over z, y, core), tp: 4 (over x).
Axes of the slice: x: 4, y: 4, z: 4, core: 2. Of those that a mesh axis runs over, the one named last changes fastest.
Arguments:
- tokens: bfloat16 [8192, 1024], P(('sp', 'tp')), may hold values from -7.5 to 7.5, as said below
- query_weight: bfloat16 [1024, 2048], P('sp', 'tp'), may hold values from -0.1875 to 0.1875
- key_weight: bfloat16 [1024, 2048], P('sp', 'tp'), may hold values from -0.1875 to 0.1875
- value_weight: bfloat16 [1024, 2048], P('sp', 'tp'), may hold values from -0.1875 to 0.1875
- gate_weight: bfloat16 [1024, 16], P('sp', 'tp'), may hold values from -0.1875 to 0.1875
- forget_bias: float32 [16], P('tp'), may hold values from 0 to 2
- out_weight: bfloat16 [2048, 1024], P('tp', 'sp'), may hold values from -0.125 to 0.125
- out_gain: float32 [1024], replicated, may hold values from 0.5 to 1.5
Outputs:
- mixed: bfloat16 [8192, 1024], P(('sp', 'tp'))
The draws below stay inside these ranges and needn't reach their ends.
Inputs may be any that keep to these rules, and one draw needn't show every extreme that they name: `tokens`: each entry is a bounded noise value (at most 6 in size) plus an offset in -1.5 to 1.5 shared by the 256 rows of one index of sp, so every entry lies within -7.5 and 7.5.
All inputs are finite; a program needn't handle non-finite values.
Results may differ from the reference program's by a relative error of at most 0.006.
Values may be sent and summed in bfloat16 or wider, within the bound.
No kernel may reach another device: no remote copies, remote signals or barrier semaphores. Data moves between devices by JAX's collectives and lax.ppermute only.
A program may use at most 128 MiB of HBM per device.

```python
import math
import jax
import jax.numpy as jnp
from jax import lax

D = 1024
HEADS = 16
HEAD_DIM = 128
TOK_DEV = 256
WIDTH = 2048
SEQ = 8192


def draw_tokens(key, part):
    noise_key = jax.random.fold_in(key, 11)
    shift_key = jax.random.fold_in(key, 12)
    noise = jax.random.truncated_normal(noise_key, -6.0, 6.0, (SEQ, D), jnp.float32)
    shifts = jax.random.uniform(shift_key, (SEQ // TOK_DEV, D), jnp.float32, -1.5, 1.5)
    return (noise + jnp.repeat(shifts, TOK_DEV, axis=0)).astype(jnp.bfloat16)


def block_scale(stream_key, extent, cuts, low, top_value):
    level = 1.0
    for dim, shards_of in cuts:
        draws = jax.random.uniform(jax.random.fold_in(jax.random.fold_in(stream_key, 6), dim), (shards_of,), jnp.float32, low / len(cuts), top_value / len(cuts))
        level = level * jnp.repeat(jnp.exp(draws), extent[dim] // shards_of).reshape((-1,) + (1,) * (len(extent) - 1 - dim))
    return level


def gaussian(own_key, dims, width, most, cuts=(), kind=jnp.bfloat16):
    factor_of = block_scale(own_key, dims, cuts, -0.22, 0.18) if cuts else 1.0
    values = jax.random.normal(own_key, dims, jnp.float32) * width * factor_of
    return jnp.minimum(jnp.maximum(values, -most), most).astype(kind)


def setup_inputs(seed: int = 0) -> dict:
    key_of = jax.random.split(jax.random.key(seed), 9)
    tokens = draw_tokens(jax.random.fold_in(key_of[8], 71), 0)
    query_weight = gaussian(key_of[1], (D, WIDTH), D ** -0.5, 0.1875, ((0, 32), (1, 4)))
    key_weight = gaussian(key_of[2], (D, WIDTH), D ** -0.5, 0.1875, ((0, 32), (1, 4)))
    value_weight = gaussian(key_of[3], (D, WIDTH), D ** -0.5, 0.1875, ((0, 32), (1, 4)))
    gate_weight = gaussian(key_of[4], (D, HEADS), D ** -0.5, 0.1875, ((0, 32), (1, 4)))
    forget_bias = jnp.clip(2.0 * jax.random.uniform(key_of[5], (HEADS,), jnp.float32) ** block_scale(key_of[5], (HEADS,), ((0, 4),), -0.2, 0.2), 0.0, 2.0)
    out_weight = gaussian(key_of[6], (WIDTH, D), WIDTH ** -0.5, 0.125, ((0, 4), (1, 32)))
    out_gain = jnp.clip(1.0 + 0.1 * jax.random.normal(key_of[7], (D,), jnp.float32), 0.5, 1.5)
    return {"tokens": tokens, "query_weight": query_weight, "key_weight": key_weight, "value_weight": value_weight, "gate_weight": gate_weight, "forget_bias": forget_bias, "out_weight": out_weight, "out_gain": out_gain}


def reference(tokens, query_weight, key_weight, value_weight, gate_weight, forget_bias, out_weight, out_gain):
    queries = jnp.dot(tokens, query_weight, preferred_element_type=jnp.float32).astype(jnp.bfloat16)
    keys = jnp.dot(tokens, key_weight, preferred_element_type=jnp.float32).astype(jnp.bfloat16)
    values = jnp.dot(tokens, value_weight, preferred_element_type=jnp.float32).astype(jnp.bfloat16)
    queries = queries.reshape(SEQ, HEADS, HEAD_DIM).astype(jnp.float32)
    keys = keys.reshape(SEQ, HEADS, HEAD_DIM).astype(jnp.float32)
    values = values.reshape(SEQ, HEADS, HEAD_DIM).astype(jnp.float32)
    raw_gate = jnp.dot(tokens, gate_weight, preferred_element_type=jnp.float32)
    log_gate = jax.nn.log_sigmoid(raw_gate + forget_bias + math.log(SEQ))
    cumulative = jnp.cumsum(log_gate, axis=0)
    scale = HEAD_DIM ** (-0.5)
    key_pos = jnp.arange(SEQ, dtype=jnp.int32)

    def one_block(index):
        start = (index * TOK_DEV).astype(jnp.int32)
        block_q = lax.dynamic_slice_in_dim(queries, start, TOK_DEV, 0)
        block_c = lax.dynamic_slice_in_dim(cumulative, start, TOK_DEV, 0)
        logits = jnp.einsum('qhd,khd->hqk', block_q, keys) * scale
        logits = logits + block_c.T[:, :, None] - cumulative.T[:, None, :]
        query_pos = start + jnp.arange(TOK_DEV, dtype=jnp.int32)
        allowed = key_pos[None, :] <= query_pos[:, None]
        logits = jnp.where(allowed[None], logits, -1e+30)
        weights = jax.nn.softmax(logits, axis=-1)
        result = jnp.einsum('hqk,khd->qhd', weights, values)
        return result.reshape(TOK_DEV, WIDTH).astype(jnp.bfloat16)
    attended = lax.map(one_block, jnp.arange(SEQ // TOK_DEV, dtype=jnp.int32)).reshape(SEQ, WIDTH)
    summed = jnp.dot(attended, out_weight, preferred_element_type=jnp.float32)
    normed = summed * lax.rsqrt(lax.optimization_barrier(jnp.mean(summed * summed, axis=-1, keepdims=True)) + 1e-06)
    return (normed * out_gain).astype(jnp.bfloat16)
```

```python
import functools
import math

import jax
import jax.numpy as jnp
from jax import lax
from jax.experimental import pallas as pl
from jax.experimental.pallas import tpu as pltpu
from jax.sharding import Mesh
from jax.sharding import PartitionSpec as P


BF = jnp.bfloat16
F32 = jnp.float32
LOG2E = math.log2(math.e)
NEG = -1e30
VMEM = pl.BlockSpec(memory_space=pltpu.VMEM)
SMEM = pl.BlockSpec(memory_space=pltpu.SMEM)


def call(body, outs, n_in, scratch=(), name=None):
    return pl.pallas_call(
        body,
        out_shape=outs,
        in_specs=[SMEM] + [VMEM] * (n_in - 1),
        out_specs=jax.tree.map(lambda _: VMEM, outs),
        scratch_shapes=list(scratch),
        compiler_params=pltpu.CompilerParams(vmem_limit_bytes=56 * 1024 * 1024),
        name=name,
    )


def around(axis, shift, value, size):
    return lax.ppermute(value, axis, [(i, (i + shift) % size) for i in range(size)])


def slot_of(index, shift, size):
    return lax.rem(index + (size - shift), size)


def pack_body(at, tok, wq, wk, wv, gate, ow, *outs):
    z = at[0]
    lane4 = lax.broadcasted_iota(jnp.int32, (32, 4), 1)
    lane = lax.broadcasted_iota(jnp.int32, (32, 128), 1)
    rows = lax.broadcasted_iota(jnp.int32, (128, 128), 0)
    cols = lax.broadcasted_iota(jnp.int32, (128, 128), 1)
    eye = (rows == cols).astype(BF)
    turned = [
        lax.dot_general(
            ow[i * 128 : (i + 1) * 128, :], eye, (((0,), (0,)), ((), ())),
            preferred_element_type=F32,
        ).astype(BF)
        for i in range(4)
    ]
    gates = gate[...].astype(F32)
    for s in range(4):
        head = lax.rem(z + s, 4)
        o = outs[s]
        o[0:64, :] = tok[:, 512:1024]
        take = pl.ds(pl.multiple_of(head * 128, 128), 128)
        o[64:96, 0:128] = wq[:, take]
        o[64:96, 128:256] = wk[:, take]
        o[64:96, 256:384] = wv[:, take]
        column = jnp.sum(jnp.where(lane4 == head, gates, 0.0), axis=1, keepdims=True)
        o[64:96, 384:512] = jnp.where(lane == 0, column, 0.0).astype(BF)
        for i in range(4):
            o[96:128, i * 128 : (i + 1) * 128] = turned[i]
    outs[4][...] = tok[:, 0:512]


def project_body(seq_len, at, bias, *refs):
    a_half, b_half, own_w, other_w = refs[0:4], refs[4:8], refs[8:12], refs[12:16]
    q_out, kv_out, cum_out = refs[16:19]
    toks, weights, gates = refs[19:]
    z, y, c, x = at[0], at[1], at[2], at[3]
    for s in range(4):
        zs = slot_of(z, s, 4)
        for i in range(4):
            xs = slot_of(x, i, 4)
            place = pl.ds(pl.multiple_of((zs * 4 + xs) * 64, 64), 64)
            toks[place, 0:512] = a_half[s][i * 64 : (i + 1) * 64, :]
            toks[place, 512:1024] = b_half[i][s * 64 : (s + 1) * 64, :]
        for j in range(4):
            ys = slot_of(y, j, 4)
            for k, w in ((c, own_w[j]), (1 - c, other_w[j])):
                place = pl.ds(pl.multiple_of((zs * 8 + ys * 2 + k) * 32, 32), 32)
                weights[place, :] = w[s * 64 : s * 64 + 32, :]
    whole = weights[...]
    for r in range(4):
        part = slice(r * 256, (r + 1) * 256)
        got = jnp.dot(toks[part, :], whole, preferred_element_type=F32)
        q_out[part, :] = got[:, 0:128].astype(BF)
        kv_out[part, :] = got[:, 128:384].astype(BF)
        gates[r : r + 1, :] = got[:, 384:512].T[0:1, :]
    gates[4:8, :] = jnp.zeros((4, 256), F32)
    v = gates[...] + bias[0:1, 0:1] + math.log(seq_len)
    u = jnp.exp(-jnp.abs(v))
    w1 = 1.0 + u
    soft = jnp.where(w1 == 1.0, u, jnp.log(w1) * (u / jnp.where(w1 == 1.0, 1.0, w1 - 1.0)))
    logs = jnp.minimum(v, 0.0) - soft
    upper = (
        lax.broadcasted_iota(jnp.int32, (256, 256), 0)
        <= lax.broadcasted_iota(jnp.int32, (256, 256), 1)
    ).astype(BF)
    total = jnp.zeros((8, 256), F32)
    for piece in in_parts(logs):
        total = total + jnp.dot(piece, upper, preferred_element_type=F32)
    pieces = in_parts(total)
    cum_out[0:16, :] = jnp.concatenate([pieces[0].astype(F32), pieces[1].astype(F32)]).astype(BF)
    cum_out[16:32, :] = jnp.concatenate(
        [pieces[2].astype(F32), jnp.zeros((8, 256), F32)]
    ).astype(BF)


def in_parts(value):
    high = value.astype(BF)
    rest = value - high.astype(F32)
    middle = rest.astype(BF)
    low = (rest - middle.astype(F32)).astype(BF)
    return high, middle, low


def attend_body(slots, first, last, scale, at, q, cum_own, cum_other, *refs):
    n = len(slots)
    kvs, refs = refs[:n], refs[n:]
    if first:
        m_in = acc_in = None
    else:
        m_in, acc_in = refs[:2]
        refs = refs[2:]
    if last:
        (out,) = refs[:1]
        refs = refs[1:]
    else:
        m_out, acc_out = refs[:2]
        refs = refs[2:]
    k_all, v_all, scores, probs = refs
    y, c = at[1], at[2]
    place = {}
    local = {}
    for own in (True, False):
        ref = cum_own if own else cum_other
        for j in range(4):
            got = ref[j * 32 : (j + 1) * 32, :].astype(F32)
            local[own, j] = got[0:8] + got[8:16] + got[16:24]
            place[own, j] = slot_of(y, j, 4) * 2 + (c if own else 1 - c)
    ends = {s: local[s][:, 255:256] for s in local}
    row = lax.broadcasted_iota(jnp.int32, (8, 1), 0)
    every = functools.reduce(jnp.add, ends.values())
    before = jnp.zeros((8, 1), F32)
    for i in range(3):
        before = before + jnp.where(row > i, every[i : i + 1, :], 0.0)

    def absolute(s):
        inner = before
        for t in ends:
            inner = inner + jnp.where(place[t] < place[s], ends[t], 0.0)
        return (local[s] + inner) * LOG2E

    here = place[True, 0]
    own_cum = absolute((True, 0))
    bias_full, bias_edge = [], []
    for s in slots:
        b = own_cum if s == (True, 0) else absolute(s)
        bias_full.append(b)
        bias_edge.append(b if s == (True, 0) else jnp.where(place[s] < here, b, -NEG))
    ones = jnp.ones((256, 128), BF)
    for zk in range(4):
        for i in range(n):
            block = slice((zk * n + i) * 256, (zk * n + i + 1) * 256)
            k_all[block, :] = kvs[i][zk * 256 : (zk + 1) * 256, 0:128]
            v_all[block, 0:128] = kvs[i][zk * 256 : (zk + 1) * 256, 128:256]
            v_all[block, 128:256] = ones
    causal = lax.broadcasted_iota(jnp.int32, (256, 256), 1) <= lax.broadcasted_iota(
        jnp.int32, (256, 256), 0
    )
    for zq in range(4):
        rows = slice(zq * 256, (zq + 1) * 256)
        queries = q[rows, :]
        cum_t = jnp.broadcast_to(own_cum[zq : zq + 1, :], (128, 256)).T
        top = jnp.full((256, 128), NEG, F32)
        for zk in range(zq + 1):
            for i in range(n):
                block = slice((zk * n + i) * 256, (zk * n + i + 1) * 256)
                bias = (bias_edge if zk == zq else bias_full)[i][zk : zk + 1, :]
                got = (
                    lax.dot_general(
                        queries, k_all[block, :], (((1,), (1,)), ((), ())),
                        preferred_element_type=F32,
                    )
                    * (scale * LOG2E)
                    - bias
                )
                if zk == zq and slots[i] == (True, 0):
                    got = jnp.where(causal, got, NEG)
                scores[:, block] = got
                top = jnp.maximum(top, jnp.maximum(got[:, 0:128], got[:, 128:256]))
        peak = jnp.broadcast_to(jnp.max(top, axis=1, keepdims=True), (256, 128)) + cum_t
        if not first:
            old = m_in[rows, :]
            peak = jnp.maximum(peak, old)
        shift = cum_t - peak
        shift = jnp.concatenate([shift, shift], axis=1)
        for b in range((zq + 1) * n):
            block = slice(b * 256, (b + 1) * 256)
            probs[:, block] = jnp.exp2(scores[:, block] + shift).astype(BF)
        width = (zq + 1) * n * 256
        acc = jnp.dot(probs[:, 0:width], v_all[0:width, :], preferred_element_type=F32)
        if not first:
            factor = jnp.exp2(old - peak)
            acc = acc + acc_in[rows, :] * jnp.concatenate([factor, factor], axis=1)
        if last:
            out[rows, :] = (acc[:, 0:128] / acc[:, 128:256]).astype(BF)
        else:
            m_out[rows, :] = peak
            acc_out[rows, :] = acc


def emit_body(at, *refs):
    att, own_w, other_w = refs[0:4], refs[4:8], refs[8:12]
    outs = refs[12:16]
    joined, weights, whole = refs[16:]
    z, y, c, x = at[0], at[1], at[2], at[3]
    for s in range(4):
        zs = slot_of(z, s, 4)
        joined[:, pl.ds(pl.multiple_of(zs * 128, 128), 128)] = att[s][...]
        for j in range(4):
            ys = slot_of(y, j, 4)
            for k, w in ((c, own_w[j]), (1 - c, other_w[j])):
                place = pl.ds(pl.multiple_of((zs * 8 + ys * 2 + k) * 32, 32), 32)
                weights[place, :] = w[s * 64 + 32 : s * 64 + 64, :]
    whole[...] = lax.dot_general(
        joined[...], weights[...], (((1,), (1,)), ((), ())), preferred_element_type=F32
    )
    for s in range(4):
        xs = lax.rem(x + s, 4)
        got = whole[pl.ds(pl.multiple_of(xs * 64, 64), 64), :]
        outs[s][...] = got.astype(outs[s].dtype)


def finish_body(at, own, r1, r2, r3, gain, out):
    total = own[...] + r1[...].astype(F32) + r2[...].astype(F32) + r3[...].astype(F32)
    mean = jnp.mean(total * total, axis=1, keepdims=True)
    out[...] = (total * lax.rsqrt(mean + 1e-06) * gain[...]).astype(BF)


def shape(*dims, dtype=BF):
    return jax.ShapeDtypeStruct(dims, dtype)


def local(tokens, wq, wk, wv, gate, forget_bias, out_weight, out_gain):
    z, y = lax.axis_index("z"), lax.axis_index("y")
    c, x = lax.axis_index("c"), lax.axis_index("x")
    at = jnp.stack([z, y, c, x]).astype(jnp.int32)
    bias = lax.dynamic_slice_in_dim(forget_bias, z, 1, 0).reshape(1, 1)
    seq_len = tokens.shape[0] * 128

    *first, a_own = call(
        pack_body, [shape(128, 512)] * 4 + [shape(64, 512)], 7, name="pack"
    )(at, tokens, wq, wk, wv, gate, out_weight)
    by_z = [first[0]] + [around("z", s, first[s], 4) for s in (1, 2, 3)]
    a_x = [a_own] + [around("x", s, a_own, 4) for s in (1, 2, 3)]

    mine = jnp.concatenate([m[64:128] for m in by_z], axis=0)
    own_w = [mine] + [around("y", s, mine, 4) for s in (1, 2, 3)]
    a4 = jnp.concatenate(a_x, axis=0)
    b4 = jnp.concatenate([m[0:64] for m in by_z], axis=0)
    a_half = [a4] + [around("z", s, a4, 4) for s in (1, 2, 3)]
    b_half = [b4] + [around("x", s, b4, 4) for s in (1, 2, 3)]
    other_w = [around("c", 1, w, 2) for w in own_w]

    q, kv, cum = call(
        functools.partial(project_body, seq_len),
        [shape(1024, 128), shape(1024, 256), shape(32, 256)],
        18,
        [
            pltpu.VMEM((1024, 1024), BF),
            pltpu.VMEM((1024, 512), BF),
            pltpu.VMEM((8, 256), F32),
        ],
        name="project",
    )(at, bias, *a_half, *b_half, *own_w, *other_w)

    cum_own = jnp.concatenate([cum] + [around("y", s, cum, 4) for s in (1, 2, 3)], axis=0)
    cum_other = around("c", 1, cum_own, 2)
    kv_own = [kv] + [around("y", s, kv, 4) for s in (1, 3, 2)]
    kv_own = [kv_own[0], kv_own[1], kv_own[3], kv_own[2]]
    kv_other = [around("c", 1, m, 2) for m in kv_own]
    where = {(True, j): kv_own[j] for j in range(4)} | {(False, j): kv_other[j] for j in range(4)}

    groups = (
        ((True, 0), (False, 0)),
        ((True, 1), (False, 1), (True, 3), (False, 3)),
        ((True, 2), (False, 2)),
    )
    state = ()
    for g, slots in enumerate(groups):
        n = len(slots)
        first_call, last_call = g == 0, g == len(groups) - 1
        outs = (
            [shape(1024, 128)]
            if last_call
            else [shape(1024, 128, dtype=F32), shape(1024, 256, dtype=F32)]
        )
        state = call(
            functools.partial(attend_body, slots, first_call, last_call, 128 ** -0.5),
            outs,
            4 + n + (0 if first_call else 2),
            [
                pltpu.VMEM((n * 1024, 128), BF),
                pltpu.VMEM((n * 1024, 256), BF),
                pltpu.VMEM((256, n * 1024), F32),
                pltpu.VMEM((256, n * 1024), BF),
            ],
            name=f"attend_{g}",
        )(at, q, cum_own, cum_other, *[where[s] for s in slots], *state)
    (attended,) = state

    def chunk(s):
        return lax.dynamic_slice_in_dim(attended, lax.rem(z + s, 4) * 256, 256, 0)

    att = [chunk(0)] + [around("z", s, chunk(s), 4) for s in (1, 2, 3)]
    own, *rest = call(
        emit_body,
        [shape(64, 1024, dtype=F32)] + [shape(64, 1024)] * 3,
        13,
        [
            pltpu.VMEM((256, 512), BF),
            pltpu.VMEM((1024, 512), BF),
            pltpu.VMEM((256, 1024), F32),
        ],
        name="emit",
    )(at, *att, *own_w, *other_w)
    got = [around("x", s, rest[s - 1], 4) for s in (1, 2, 3)]
    (out,) = call(finish_body, [shape(64, 1024)], 6, name="finish")(
        at, own, *got, out_gain.reshape(1, 1024)
    )
    return out


def solution(mesh):
    torus = Mesh(mesh.devices.reshape(4, 4, 2, 4), ("z", "y", "c", "x"))
    sp = ("z", "y", "c")
    in_specs = (
        P(sp + ("x",), None),
        P(sp, "x"),
        P(sp, "x"),
        P(sp, "x"),
        P(sp, "x"),
        P("x"),
        P("x", sp),
        P(),
    )
    return jax.shard_map(
        local, mesh=torus, in_specs=in_specs, out_specs=P(sp + ("x",), None), check_vma=False
    )
```

```python
import functools
import math

import jax
import jax.numpy as jnp
from jax import lax
from jax.experimental import pallas as pl
from jax.experimental.pallas import tpu as pltpu
from jax.sharding import Mesh
from jax.sharding import PartitionSpec as P


BF = jnp.bfloat16
F32 = jnp.float32
LOG2E = math.log2(math.e)
NEG = -1e30
VMEM = pl.BlockSpec(memory_space=pltpu.VMEM)
SMEM = pl.BlockSpec(memory_space=pltpu.SMEM)


def kept(value):
    return pltpu.with_memory_space_constraint(value, pltpu.VMEM)


def named(body, outs, scratch=(), mib=20, first=False, last=False):
    def run(at, *operands):
        return pl.pallas_call(
            body,
            out_shape=outs if last else [pltpu.VMEM(o.shape, o.dtype) for o in outs],
            in_specs=[SMEM] + [VMEM] * len(operands),
            out_specs=[VMEM] * len(outs),
            scratch_shapes=list(scratch),
            compiler_params=pltpu.CompilerParams(vmem_limit_bytes=mib * 1024 * 1024),
        )(at, *(operands if first else map(kept, operands)))

    return run


def around(axis, shift, value, size):
    return lax.ppermute(value, axis, [(i, (i + shift) % size) for i in range(size)])


def along(axis, step, value):
    names, index = ((axis, "c"), lambda i, c: 2 * (i % 4) + c)
    if axis == "x":
        names, index = (("c", "x"), lambda i, c: 4 * c + i % 4)
    pairs = [
        (index(i, c), index(i + (step, -step)[c], c)) for i in range(4) for c in range(2)
    ]
    return lax.ppermute(value, names, pairs)


def spread(axis, value):
    first = along(axis, 1, value)
    second = along(axis, -1, value)
    return [value, first, second, along(axis, 1, first)]


def near(index, core, slot):
    return lax.rem(index + (0, 3 + 2 * core, 1 + 2 * core, 2)[slot], 4)


def slot_of(index, shift, size):
    return lax.rem(index + (size - shift), size)


def pack_body(at, tok, wq, wk, wv, gate, ow, *outs):
    z = at[0]
    row4 = lax.broadcasted_iota(jnp.int32, (4, 32), 0)
    lane = lax.broadcasted_iota(jnp.int32, (32, 128), 1)
    gates = gate[...].astype(F32)
    for s in range(4):
        head = lax.rem(z + s, 4)
        o = outs[s]
        o[0:64, :] = tok[:, 512:1024]
        take = pl.ds(pl.multiple_of(head * 128, 128), 128)
        o[64:96, 0:128] = wq[:, take]
        o[64:96, 128:256] = wk[:, take]
        o[64:96, 256:384] = wv[:, take]
        line = jnp.sum(jnp.where(row4 == head, gates, 0.0), axis=0, keepdims=True)
        column = jnp.broadcast_to(line, (128, 32)).T
        o[64:96, 384:512] = jnp.where(lane == 0, column, 0.0).astype(BF)
        o[96:128, :] = ow[...]
    outs[4][...] = tok[:, 0:512]


def w_slots(refs):
    own = [(refs[j], 0) for j in range(4)]
    other = [(refs[4], 0)] + [(refs[5], 256 * j) for j in range(3)]
    return own, other


def project_body(seq_len, at, bias, *refs):
    a_half, b_half = refs[0:4], refs[4:8]
    own_w, other_w = w_slots(refs[8:14])
    q_out, kv_out, cum_out = refs[14:17]
    toks, weights, gates = refs[17:]
    z, y, c, x = at[0], at[1], at[2], at[3]
    for s in range(4):
        zs = slot_of(z, s, 4)
        zn = near(z, c, s)
        for i in range(4):
            xs = near(x, c, i)
            place = pl.ds(pl.multiple_of((zn * 4 + xs) * 64, 64), 64)
            toks[place, 0:512] = a_half[s][i * 64 : (i + 1) * 64, :]
            place = pl.ds(pl.multiple_of((zs * 4 + xs) * 64, 64), 64)
            toks[place, 512:1024] = b_half[i][s * 64 : (s + 1) * 64, :]
        for j in range(4):
            for k, (w, at_row) in ((c, own_w[j]), (1 - c, other_w[j])):
                ys = near(y, k, j)
                place = pl.ds(pl.multiple_of((zs * 8 + ys * 2 + k) * 32, 32), 32)
                weights[place, :] = w[at_row + s * 64 : at_row + s * 64 + 32, :]
    whole = weights[...]
    for r in range(4):
        part = slice(r * 256, (r + 1) * 256)
        got = jnp.dot(toks[part, :], whole, preferred_element_type=F32)
        q_out[part, :] = got[:, 0:128].astype(BF)
        kv_out[part, :] = got[:, 128:384].astype(BF)
        gates[r : r + 1, :] = got[:, 384:512].T[0:1, :]
    gates[4:8, :] = jnp.zeros((4, 256), F32)
    v = gates[...] + bias[0:1, 0:1] + math.log(seq_len)
    u = jnp.exp(-jnp.abs(v))
    w1 = 1.0 + u
    soft = jnp.where(w1 == 1.0, u, jnp.log(w1) * (u / jnp.where(w1 == 1.0, 1.0, w1 - 1.0)))
    logs = jnp.minimum(v, 0.0) - soft
    upper = (
        lax.broadcasted_iota(jnp.int32, (256, 256), 0)
        <= lax.broadcasted_iota(jnp.int32, (256, 256), 1)
    ).astype(BF)
    total = jnp.zeros((8, 256), F32)
    for piece in in_parts(logs):
        total = total + jnp.dot(piece, upper, preferred_element_type=F32)
    pieces = in_parts(total)
    cum_out[0:16, :] = jnp.concatenate([pieces[0].astype(F32), pieces[1].astype(F32)]).astype(BF)
    cum_out[16:32, :] = jnp.concatenate(
        [pieces[2].astype(F32), jnp.zeros((8, 256), F32)]
    ).astype(BF)


def in_parts(value):
    high = value.astype(BF)
    rest = value - high.astype(F32)
    middle = rest.astype(BF)
    low = (rest - middle.astype(F32)).astype(BF)
    return high, middle, low


def attend_body(slots, first, last, scale, at, q, cum_own, cum_other, *refs):
    n = len(slots)
    kvs, refs = refs[:n], refs[n:]
    if first:
        m_in = acc_in = None
    else:
        m_in, acc_in = refs[:2]
        refs = refs[2:]
    if last:
        chunks = refs[:4]
        refs = refs[4:]
    else:
        m_out, acc_out = refs[:2]
        refs = refs[2:]
    k_all, v_all, scores, probs = refs
    y, c = at[1], at[2]
    place = {}
    local = {}
    for own in (True, False):
        ref = cum_own if own else cum_other
        for j in range(4):
            got = ref[j * 32 : (j + 1) * 32, :].astype(F32)
            local[own, j] = got[0:8] + got[8:16] + got[16:24]
            core = c if own else 1 - c
            place[own, j] = near(y, core, j) * 2 + core
    ends = {s: local[s][:, 255:256] for s in local}
    row = lax.broadcasted_iota(jnp.int32, (8, 1), 0)
    every = functools.reduce(jnp.add, ends.values())
    before = jnp.zeros((8, 1), F32)
    for i in range(3):
        before = before + jnp.where(row > i, every[i : i + 1, :], 0.0)

    def absolute(s):
        inner = before
        for t in ends:
            inner = inner + jnp.where(place[t] < place[s], ends[t], 0.0)
        return (local[s] + inner) * LOG2E

    here = place[True, 0]
    own_cum = absolute((True, 0))
    bias_full, bias_edge = [], []
    for s in slots:
        b = own_cum if s == (True, 0) else absolute(s)
        bias_full.append(b)
        bias_edge.append(b if s == (True, 0) else jnp.where(place[s] < here, b, -NEG))
    ones = jnp.ones((256, 128), BF)
    for zk in range(4):
        for i in range(n):
            block = slice((zk * n + i) * 256, (zk * n + i + 1) * 256)
            k_all[block, :] = kvs[i][zk * 256 : (zk + 1) * 256, 0:128]
            v_all[block, 0:128] = kvs[i][zk * 256 : (zk + 1) * 256, 128:256]
            v_all[block, 128:256] = ones
    causal = lax.broadcasted_iota(jnp.int32, (256, 256), 1) <= lax.broadcasted_iota(
        jnp.int32, (256, 256), 0
    )
    for zq in range(4):
        rows = slice(zq * 256, (zq + 1) * 256)
        queries = q[rows, :]
        cum_t = jnp.broadcast_to(own_cum[zq : zq + 1, :], (128, 256)).T
        top = jnp.full((256, 128), NEG, F32)
        for zk in range(zq + 1):
            for i in range(n):
                block = slice((zk * n + i) * 256, (zk * n + i + 1) * 256)
                bias = (bias_edge if zk == zq else bias_full)[i][zk : zk + 1, :]
                got = (
                    lax.dot_general(
                        queries, k_all[block, :], (((1,), (1,)), ((), ())),
                        preferred_element_type=F32,
                    )
                    * (scale * LOG2E)
                    - bias
                )
                if zk == zq and slots[i] == (True, 0):
                    got = jnp.where(causal, got, NEG)
                scores[:, block] = got
                top = jnp.maximum(top, jnp.maximum(got[:, 0:128], got[:, 128:256]))
        peak = jnp.broadcast_to(jnp.max(top, axis=1, keepdims=True), (256, 128)) + cum_t
        if not first:
            old = m_in[rows, :]
            peak = jnp.maximum(peak, old)
        shift = cum_t - peak
        shift = jnp.concatenate([shift, shift], axis=1)
        for b in range((zq + 1) * n):
            block = slice(b * 256, (b + 1) * 256)
            probs[:, block] = jnp.exp2(scores[:, block] + shift).astype(BF)
        width = (zq + 1) * n * 256
        acc = jnp.dot(probs[:, 0:width], v_all[0:width, :], preferred_element_type=F32)
        if not first:
            factor = jnp.exp2(old - peak)
            acc = acc + acc_in[rows, :] * jnp.concatenate([factor, factor], axis=1)
        if last:
            done = (acc[:, 0:128] / acc[:, 128:256]).astype(BF)
            for s in range(4):

                @pl.when(lax.rem(at[0] + s, 4) == zq)
                def _(s=s, done=done):
                    chunks[s][...] = done

        else:
            m_out[rows, :] = peak
            acc_out[rows, :] = acc


def emit_body(at, *refs):
    att = refs[0:4]
    own_w, other_w = w_slots(refs[4:10])
    outs = refs[10:14]
    joined, weights, whole = refs[14:]
    z, y, c, x = at[0], at[1], at[2], at[3]
    for s in range(4):
        zs = slot_of(z, s, 4)
        joined[:, pl.ds(pl.multiple_of(zs * 128, 128), 128)] = att[s][...]
        for j in range(4):
            for k, (w, at_row) in ((c, own_w[j]), (1 - c, other_w[j])):
                ys = near(y, k, j)
                place = pl.ds(pl.multiple_of((zs * 8 + ys * 2 + k) * 32, 32), 32)
                weights[place, :] = w[at_row + s * 64 + 32 : at_row + s * 64 + 64, :]
    whole[...] = lax.dot_general(
        joined[...], weights[...], (((1,), (1,)), ((), ())), preferred_element_type=F32
    )
    for s in range(4):
        xs = lax.rem(x + s, 4)
        got = whole[pl.ds(pl.multiple_of(xs * 64, 64), 64), :]
        outs[s][...] = got.astype(outs[s].dtype)


def finish_body(at, own, r1, r2, r3, gain, out):
    total = own[...] + r1[...].astype(F32) + r2[...].astype(F32) + r3[...].astype(F32)
    mean = jnp.mean(total * total, axis=1, keepdims=True)
    out[...] = (total * lax.rsqrt(mean + 1e-06) * gain[...]).astype(BF)


def shape(*dims, dtype=BF):
    return jax.ShapeDtypeStruct(dims, dtype)


TURN = (1, 3, 2)


def ring(axis, values):
    got = [values[0], None, None, None]
    for s in TURN:
        got[s] = around(axis, s, values[s], 4)
    return got


GROUPS = (
    ((True, 0), (False, 0)),
    ((True, 1), (False, 1), (True, 2), (False, 2)),
    ((True, 3),),
    ((False, 3),),
)


def layer(tokens, wq, wk, wv, gate, forget_bias, out_weight, out_gain):
    z, y = lax.axis_index("z"), lax.axis_index("y")
    c, x = lax.axis_index("c"), lax.axis_index("x")
    at = jnp.stack([z, y, c, x]).astype(jnp.int32)
    bias = lax.dynamic_slice_in_dim(forget_bias, z, 1, 0).reshape(1, 1)
    seq_len = tokens.shape[0] * 128

    *first, a_own = named(pack_body, [shape(128, 512)] * 4 + [shape(64, 512)], first=True)(
        at, tokens, wq, wk, wv, gate.T, out_weight.T
    )
    a_x = spread("x", a_own)
    by_z = ring("z", first)

    mine = jnp.concatenate([m[64:128] for m in by_z], axis=0)
    own_w = spread("y", mine)
    b_half = spread("x", jnp.concatenate([m[0:64] for m in by_z], axis=0))
    a_half = spread("z", jnp.concatenate(a_x, axis=0))
    other_w = [
        around("c", 1, mine, 2), around("c", 1, jnp.concatenate(own_w[1:], axis=0), 2)
    ]

    q, kv, cum = named(
        functools.partial(project_body, seq_len),
        [shape(1024, 128), shape(1024, 256), shape(32, 256)],
        [
            pltpu.VMEM((1024, 1024), BF),
            pltpu.VMEM((1024, 512), BF),
            pltpu.VMEM((8, 256), F32),
        ],
    )(at, bias, *a_half, *b_half, *own_w, *other_w)

    cum_own = jnp.concatenate(spread("y", cum), axis=0)
    cum_other = around("c", 1, cum_own, 2)
    kv_own = spread("y", kv)
    where = {(True, j): kv_own[j] for j in range(4)}
    where |= {(False, j): around("c", 1, kv_own[j], 2) for j in range(4)}

    state = ()
    for g, slots in enumerate(GROUPS):
        n = len(slots)
        first_call, last_call = g == 0, g == len(GROUPS) - 1
        outs = (
            [shape(256, 128)] * 4
            if last_call
            else [shape(1024, 128, dtype=F32), shape(1024, 256, dtype=F32)]
        )
        state = named(
            functools.partial(attend_body, slots, first_call, last_call, 128 ** -0.5),
            outs,
            [
                pltpu.VMEM((n * 1024, 128), BF),
                pltpu.VMEM((n * 1024, 256), BF),
                pltpu.VMEM((256, n * 1024), F32),
                pltpu.VMEM((256, n * 1024), BF),
            ],
        )(at, q, cum_own, cum_other, *[where[s] for s in slots], *state)

    att = ring("z", state)
    own, *rest = named(
        emit_body,
        [shape(64, 1024, dtype=F32)] + [shape(64, 1024)] * 3,
        [
            pltpu.VMEM((256, 512), BF),
            pltpu.VMEM((1024, 512), BF),
            pltpu.VMEM((256, 1024), F32),
        ],
    )(at, *att, *own_w, *other_w)
    got = ring("x", [own, *rest])
    (out,) = named(finish_body, [shape(64, 1024)], last=True)(
        at, *got, out_gain.reshape(1, 1024)
    )
    return out


def solution(mesh):
    torus = Mesh(mesh.devices.reshape(4, 4, 2, 4), ("z", "y", "c", "x"))
    sp = ("z", "y", "c")
    in_specs = (
        P(sp + ("x",), None),
        P(sp, "x"),
        P(sp, "x"),
        P(sp, "x"),
        P(sp, "x"),
        P("x"),
        P("x", sp),
        P(),
    )
    return jax.shard_map(
        layer, mesh=torus, in_specs=in_specs, out_specs=P(sp + ("x",), None), check_vma=False
    )
```

```python
import functools
import math

import jax
import jax.numpy as jnp
from jax import lax
from jax.experimental import pallas as pl
from jax.experimental.pallas import tpu as pltpu
from jax.sharding import Mesh
from jax.sharding import PartitionSpec as P


BF = jnp.bfloat16
F32 = jnp.float32
LOG2E = math.log2(math.e)
NEG = -1e30
VMEM = pl.BlockSpec(memory_space=pltpu.VMEM)
SMEM = pl.BlockSpec(memory_space=pltpu.SMEM)


def named(body, outs, scratch=(), mib=20, first=False, last=False):
    space = pltpu.HBM if first else pltpu.VMEM

    def run(at, *operands):
        return pl.pallas_call(
            body,
            out_shape=outs if last else [pltpu.VMEM(o.shape, o.dtype) for o in outs],
            in_specs=[SMEM] + [VMEM] * len(operands),
            out_specs=[VMEM] * len(outs),
            scratch_shapes=list(scratch),
            compiler_params=pltpu.CompilerParams(vmem_limit_bytes=mib * 1024 * 1024),
        )(at, *(pltpu.with_memory_space_constraint(o, space) for o in operands))

    return run


def around(axis, shift, value, size):
    return lax.ppermute(value, axis, [(i, (i + shift) % size) for i in range(size)])


def along(axis, step, value):
    names, index = ((axis, "c"), lambda i, c: 2 * (i % 4) + c)
    if axis == "x":
        names, index = (("c", "x"), lambda i, c: 4 * c + i % 4)
    pairs = [
        (index(i, c), index(i + (step, -step)[c], c)) for i in range(4) for c in range(2)
    ]
    return lax.ppermute(value, names, pairs)


def spread(axis, value, back=False):
    first = along(axis, 1, value)
    second = along(axis, -1, value)
    step, passed = (-1, second) if back else (1, first)
    return [value, first, second, along(axis, step, passed)]


def near(index, core, slot):
    return lax.rem(index + (0, 3 + 2 * core, 1 + 2 * core, 2)[slot], 4)


def slot_of(index, shift, size):
    return lax.rem(index + (size - shift), size)


def pack_body(at, tok, wq, wk, wv, gate, ow, *outs):
    z = at[0]
    row4 = lax.broadcasted_iota(jnp.int32, (4, 32), 0)
    lane = lax.broadcasted_iota(jnp.int32, (32, 128), 1)
    gates = gate[...].astype(F32)
    for s in range(4):
        head = lax.rem(z + s, 4)
        o = outs[s]
        o[0:64, :] = tok[:, 512:1024]
        take = pl.ds(pl.multiple_of(head * 128, 128), 128)
        o[64:96, 0:128] = wq[:, take]
        o[64:96, 128:256] = wk[:, take]
        o[64:96, 256:384] = wv[:, take]
        line = jnp.sum(jnp.where(row4 == head, gates, 0.0), axis=0, keepdims=True)
        column = jnp.broadcast_to(line, (128, 32)).T
        o[64:96, 384:512] = jnp.where(lane == 0, column, 0.0).astype(BF)
        o[96:128, :] = ow[...]
    outs[4][...] = tok[:, 0:512]


def project_body(seq_len, at, *refs):
    bias, refs = refs[0], refs[1:]
    a_half, b_half = refs[0:4], refs[4:8]
    own_w, other_w = refs[8:12], refs[12:16]
    q_out, kv_out, cum_out = refs[16:19]
    toks, weights, gates = refs[19:]
    z, y, c, x = at[0], at[1], at[2], at[3]
    for s in range(4):
        zs = slot_of(z, s, 4)
        zn = near(z, c, s)
        for i in range(4):
            xs = near(x, c, i)
            place = pl.ds(pl.multiple_of((zn * 4 + xs) * 64, 64), 64)
            toks[place, 0:512] = a_half[s][i * 64 : (i + 1) * 64, :]
            place = pl.ds(pl.multiple_of((zs * 4 + xs) * 64, 64), 64)
            toks[place, 512:1024] = b_half[i][s * 64 : (s + 1) * 64, :]
        for j in range(4):
            for k, w in ((c, own_w[j]), (1 - c, other_w[j])):
                ys = near(y, k, j)
                place = pl.ds(pl.multiple_of((zs * 8 + ys * 2 + k) * 32, 32), 32)
                weights[place, :] = w[s * 64 : s * 64 + 32, :]
    whole = weights[...]
    for r in range(4):
        part = slice(r * 256, (r + 1) * 256)
        got = jnp.dot(toks[part, :], whole, preferred_element_type=F32)
        q_out[part, :] = got[:, 0:128].astype(BF)
        kv_out[part, :] = got[:, 128:384].astype(BF)
        gates[r : r + 1, :] = got[:, 384:512].T[0:1, :]
    gates[4:8, :] = jnp.zeros((4, 256), F32)
    spots = lax.broadcasted_iota(jnp.int32, (1, 4), 1)
    held = jnp.sum(jnp.where(spots == z, bias[...], 0.0), axis=1, keepdims=True)
    v = gates[...] + held + math.log(seq_len)
    u = jnp.exp(-jnp.abs(v))
    w1 = 1.0 + u
    soft = jnp.where(w1 == 1.0, u, jnp.log(w1) * (u / jnp.where(w1 == 1.0, 1.0, w1 - 1.0)))
    logs = jnp.minimum(v, 0.0) - soft
    upper = (
        lax.broadcasted_iota(jnp.int32, (256, 256), 0)
        <= lax.broadcasted_iota(jnp.int32, (256, 256), 1)
    ).astype(BF)
    total = jnp.zeros((8, 256), F32)
    for piece in in_parts(logs):
        total = total + jnp.dot(piece, upper, preferred_element_type=F32)
    pieces = in_parts(total)
    cum_out[0:16, :] = jnp.concatenate([pieces[0].astype(F32), pieces[1].astype(F32)]).astype(BF)
    cum_out[16:32, :] = jnp.concatenate(
        [pieces[2].astype(F32), jnp.zeros((8, 256), F32)]
    ).astype(BF)


def in_parts(value):
    high = value.astype(BF)
    rest = value - high.astype(F32)
    middle = rest.astype(BF)
    low = (rest - middle.astype(F32)).astype(BF)
    return high, middle, low


def attend_body(slots, first, last, scale, at, q, cum_own, cum_other, *refs):
    n = len(slots)
    kvs, refs = refs[:n], refs[n:]
    if first:
        m_in = acc_in = None
    else:
        m_in, acc_in = refs[:2]
        refs = refs[2:]
    if last:
        chunks = refs[:4]
        refs = refs[4:]
    else:
        m_out, acc_out = refs[:2]
        refs = refs[2:]
    k_all, v_all, scores, probs = refs
    y, c = at[1], at[2]
    place = {}
    local = {}
    for own in (True, False):
        ref = cum_own if own else cum_other
        for j in range(4):
            got = ref[j * 32 : (j + 1) * 32, :].astype(F32)
            local[own, j] = got[0:8] + got[8:16] + got[16:24]
            core = c if own else 1 - c
            place[own, j] = near(y, core, j) * 2 + core
    ends = {s: local[s][:, 255:256] for s in local}
    row = lax.broadcasted_iota(jnp.int32, (8, 1), 0)
    every = functools.reduce(jnp.add, ends.values())
    before = jnp.zeros((8, 1), F32)
    for i in range(3):
        before = before + jnp.where(row > i, every[i : i + 1, :], 0.0)

    def absolute(s):
        inner = before
        for t in ends:
            inner = inner + jnp.where(place[t] < place[s], ends[t], 0.0)
        return (local[s] + inner) * LOG2E

    here = place[True, 0]
    own_cum = absolute((True, 0))
    bias_full, bias_edge = [], []
    for s in slots:
        b = own_cum if s == (True, 0) else absolute(s)
        bias_full.append(b)
        bias_edge.append(b if s == (True, 0) else jnp.where(place[s] < here, b, -NEG))
    ones = jnp.ones((256, 128), BF)
    for zk in range(4):
        for i in range(n):
            block = slice((zk * n + i) * 256, (zk * n + i + 1) * 256)
            k_all[block, :] = kvs[i][zk * 256 : (zk + 1) * 256, 0:128]
            v_all[block, 0:128] = kvs[i][zk * 256 : (zk + 1) * 256, 128:256]
            v_all[block, 128:256] = ones
    causal = lax.broadcasted_iota(jnp.int32, (256, 256), 1) <= lax.broadcasted_iota(
        jnp.int32, (256, 256), 0
    )
    for zq in range(4):
        rows = slice(zq * 256, (zq + 1) * 256)
        queries = q[rows, :]
        cum_t = jnp.broadcast_to(own_cum[zq : zq + 1, :], (128, 256)).T
        top = jnp.full((256, 128), NEG, F32)
        for zk in range(zq + 1):
            for i in range(n):
                block = slice((zk * n + i) * 256, (zk * n + i + 1) * 256)
                bias = (bias_edge if zk == zq else bias_full)[i][zk : zk + 1, :]
                got = (
                    lax.dot_general(
                        queries, k_all[block, :], (((1,), (1,)), ((), ())),
                        preferred_element_type=F32,
                    )
                    * (scale * LOG2E)
                    - bias
                )
                if zk == zq and slots[i] == (True, 0):
                    got = jnp.where(causal, got, NEG)
                scores[:, block] = got
                top = jnp.maximum(top, jnp.maximum(got[:, 0:128], got[:, 128:256]))
        peak = jnp.broadcast_to(jnp.max(top, axis=1, keepdims=True), (256, 128)) + cum_t
        if not first:
            old = m_in[rows, :]
            peak = jnp.maximum(peak, old)
        shift = cum_t - peak
        shift = jnp.concatenate([shift, shift], axis=1)
        for b in range((zq + 1) * n):
            block = slice(b * 256, (b + 1) * 256)
            probs[:, block] = jnp.exp2(scores[:, block] + shift).astype(BF)
        width = (zq + 1) * n * 256
        acc = jnp.dot(probs[:, 0:width], v_all[0:width, :], preferred_element_type=F32)
        if not first:
            factor = jnp.exp2(old - peak)
            acc = acc + acc_in[rows, :] * jnp.concatenate([factor, factor], axis=1)
        if last:
            done = (acc[:, 0:128] / acc[:, 128:256]).astype(BF)
            for s in range(4):

                @pl.when(lax.rem(at[0] + s, 4) == zq)
                def _(s=s, done=done):
                    chunks[s][...] = done

        else:
            m_out[rows, :] = peak
            acc_out[rows, :] = acc


def emit_body(at, *refs):
    att = refs[0:4]
    own_w, other_w = refs[4:8], refs[8:12]
    outs = refs[12:16]
    joined, weights, whole = refs[16:]
    z, y, c, x = at[0], at[1], at[2], at[3]
    for s in range(4):
        zs = slot_of(z, s, 4)
        joined[:, pl.ds(pl.multiple_of(zs * 128, 128), 128)] = att[s][...]
        for j in range(4):
            for k, w in ((c, own_w[j]), (1 - c, other_w[j])):
                ys = near(y, k, j)
                place = pl.ds(pl.multiple_of((zs * 8 + ys * 2 + k) * 32, 32), 32)
                weights[place, :] = w[s * 64 + 32 : s * 64 + 64, :]
    whole[...] = lax.dot_general(
        joined[...], weights[...], (((1,), (1,)), ((), ())), preferred_element_type=F32
    )
    for s in range(4):
        xs = lax.rem(x + s, 4)
        got = whole[pl.ds(pl.multiple_of(xs * 64, 64), 64), :]
        outs[s][...] = got.astype(outs[s].dtype)


def finish_body(at, own, r1, r2, r3, gain, out):
    total = own[...] + r1[...].astype(F32) + r2[...].astype(F32) + r3[...].astype(F32)
    mean = jnp.mean(total * total, axis=1, keepdims=True)
    out[...] = (total * lax.rsqrt(mean + 1e-06) * gain[...]).astype(BF)


def shape(*dims, dtype=BF):
    return jax.ShapeDtypeStruct(dims, dtype)


TURN = (1, 3, 2)


def ring(axis, values):
    got = [values[0], None, None, None]
    for s in TURN:
        got[s] = around(axis, s, values[s], 4)
    return got


GROUPS = (
    ((True, 0), (False, 0)),
    ((True, 1), (False, 1), (True, 2), (False, 2)),
    ((True, 3),),
    ((False, 3),),
)


def layer(tokens, wq, wk, wv, gate, forget_bias, out_weight, out_gain):
    z, y = lax.axis_index("z"), lax.axis_index("y")
    c, x = lax.axis_index("c"), lax.axis_index("x")
    at = jnp.stack([z, y, c, x]).astype(jnp.int32)
    bias = forget_bias.reshape(1, 4)
    seq_len = tokens.shape[0] * 128

    *first, a_own = named(pack_body, [shape(128, 512)] * 4 + [shape(64, 512)], first=True)(
        at, tokens, wq, wk, wv, gate.T, out_weight.T
    )
    a_x = spread("x", a_own)
    by_z = ring("z", first)

    mine = jnp.concatenate([m[64:128] for m in by_z], axis=0)
    own_w = spread("y", mine)
    b_half = spread("x", jnp.concatenate([m[0:64] for m in by_z], axis=0))
    a_half = spread("z", jnp.concatenate(a_x, axis=0))
    other_w = [around("c", 1, w, 2) for w in own_w]

    q, kv, cum = named(
        functools.partial(project_body, seq_len),
        [shape(1024, 128), shape(1024, 256), shape(32, 256)],
        [
            pltpu.VMEM((1024, 1024), BF),
            pltpu.VMEM((1024, 512), BF),
            pltpu.VMEM((8, 256), F32),
        ],
    )(at, bias, *a_half, *b_half, *own_w, *other_w)

    cum_own = jnp.concatenate(spread("y", cum, back=True), axis=0)
    cum_other = around("c", 1, cum_own, 2)
    kv_own = spread("y", kv)
    where = {(True, j): kv_own[j] for j in range(4)}
    where |= {(False, j): around("c", 1, kv_own[j], 2) for j in range(4)}

    state = ()
    for g, slots in enumerate(GROUPS):
        n = len(slots)
        first_call, last_call = g == 0, g == len(GROUPS) - 1
        outs = (
            [shape(256, 128)] * 4
            if last_call
            else [shape(1024, 128, dtype=F32), shape(1024, 256, dtype=F32)]
        )
        state = named(
            functools.partial(attend_body, slots, first_call, last_call, 128 ** -0.5),
            outs,
            [
                pltpu.VMEM((n * 1024, 128), BF),
                pltpu.VMEM((n * 1024, 256), BF),
                pltpu.VMEM((256, n * 1024), F32),
                pltpu.VMEM((256, n * 1024), BF),
            ],
        )(at, q, cum_own, cum_other, *[where[s] for s in slots], *state)

    att = ring("z", state)
    own, *rest = named(
        emit_body,
        [shape(64, 1024, dtype=F32)] + [shape(64, 1024)] * 3,
        [
            pltpu.VMEM((256, 512), BF),
            pltpu.VMEM((1024, 512), BF),
            pltpu.VMEM((256, 1024), F32),
        ],
    )(at, *att, *own_w, *other_w)
    got = ring("x", [own, *rest])
    (out,) = named(finish_body, [shape(64, 1024)], last=True)(at, *got, out_gain.reshape(1, 1024))
    return out


def solution(mesh):
    torus = Mesh(mesh.devices.reshape(4, 4, 2, 4), ("z", "y", "c", "x"))
    sp = ("z", "y", "c")
    in_specs = (
        P(sp + ("x",), None),
        P(sp, "x"),
        P(sp, "x"),
        P(sp, "x"),
        P(sp, "x"),
        P("x"),
        P("x", sp),
        P(),
    )
    return jax.shard_map(
        layer, mesh=torus, in_specs=in_specs, out_specs=P(sp + ("x",), None), check_vma=False
    )
```

```python
import functools
import math

import jax
import jax.numpy as jnp
from jax import lax
from jax.experimental import pallas as pl
from jax.experimental.pallas import tpu as pltpu
from jax.sharding import Mesh
from jax.sharding import PartitionSpec as P


BF = jnp.bfloat16
F32 = jnp.float32
LOG2E = math.log2(math.e)
NEG = -1e30
VMEM = pl.BlockSpec(memory_space=pltpu.VMEM)
SMEM = pl.BlockSpec(memory_space=pltpu.SMEM)


def named(body, outs, scratch=(), mib=20, first=False, last=False):
    space = pltpu.HBM if first else pltpu.VMEM

    def run(at, *operands):
        return pl.pallas_call(
            body,
            out_shape=outs if last else [pltpu.VMEM(o.shape, o.dtype) for o in outs],
            in_specs=[SMEM] + [VMEM] * len(operands),
            out_specs=[VMEM] * len(outs),
            scratch_shapes=list(scratch),
            compiler_params=pltpu.CompilerParams(vmem_limit_bytes=mib * 1024 * 1024),
        )(at, *(pltpu.with_memory_space_constraint(o, space) for o in operands))

    return run


def around(axis, shift, value, size):
    return lax.ppermute(value, axis, [(i, (i + shift) % size) for i in range(size)])


def along(axis, step, value):
    names, index = ((axis, "c"), lambda i, c: 2 * (i % 4) + c)
    if axis == "x":
        names, index = (("c", "x"), lambda i, c: 4 * c + i % 4)
    pairs = [
        (index(i, c), index(i + (step, -step)[c], c)) for i in range(4) for c in range(2)
    ]
    return lax.ppermute(value, names, pairs)


def spread(axis, value, step=1):
    first = along(axis, step, value)
    second = along(axis, -step, value)
    pair = [first, second] if step == 1 else [second, first]
    return [value, *pair, along(axis, step, first)]


def near(index, core, slot):
    return lax.rem(index + (0, 3 + 2 * core, 1 + 2 * core, 2)[slot], 4)


def slot_of(index, shift, size):
    return lax.rem(index + (size - shift), size)


def pack_body(at, tok, wq, wk, wv, gate, ow, *outs):
    z = at[0]
    row4 = lax.broadcasted_iota(jnp.int32, (4, 32), 0)
    lane = lax.broadcasted_iota(jnp.int32, (32, 128), 1)
    gates = gate[...].astype(F32)
    for s in range(4):
        head = lax.rem(z + s, 4)
        o = outs[s]
        o[0:64, :] = tok[:, 512:1024]
        take = pl.ds(pl.multiple_of(head * 128, 128), 128)
        o[64:96, 0:128] = wq[:, take]
        o[64:96, 128:256] = wk[:, take]
        o[64:96, 256:384] = wv[:, take]
        line = jnp.sum(jnp.where(row4 == head, gates, 0.0), axis=0, keepdims=True)
        column = jnp.broadcast_to(line, (128, 32)).T
        o[64:96, 384:512] = jnp.where(lane == 0, column, 0.0).astype(BF)
        o[96:128, :] = ow[...]
    outs[4][...] = tok[:, 0:512]


def project_body(seq_len, at, *refs):
    bias, refs = refs[0], refs[1:]
    a_half, b_half = refs[0:4], refs[4:8]
    own_w, other_w = refs[8:12], refs[12:16]
    q_out, kv_out, cum_out = refs[16:19]
    toks, weights, gates = refs[19:]
    z, y, c, x = at[0], at[1], at[2], at[3]
    for s in range(4):
        zs = slot_of(z, s, 4)
        zn = near(z, c, s)
        for i in range(4):
            xs = near(x, c, i)
            place = pl.ds(pl.multiple_of((zn * 4 + xs) * 64, 64), 64)
            toks[place, 0:512] = a_half[s][i * 64 : (i + 1) * 64, :]
            place = pl.ds(pl.multiple_of((zs * 4 + xs) * 64, 64), 64)
            toks[place, 512:1024] = b_half[i][s * 64 : (s + 1) * 64, :]
        for j in range(4):
            for k, w in ((c, own_w[j]), (1 - c, other_w[j])):
                ys = near(y, k, j)
                place = pl.ds(pl.multiple_of((zs * 8 + ys * 2 + k) * 32, 32), 32)
                weights[place, :] = w[s * 64 : s * 64 + 32, :]
    whole = weights[...]
    for r in range(4):
        part = slice(r * 256, (r + 1) * 256)
        got = jnp.dot(toks[part, :], whole, preferred_element_type=F32)
        q_out[part, :] = got[:, 0:128].astype(BF)
        kv_out[part, :] = got[:, 128:384].astype(BF)
        gates[r : r + 1, :] = got[:, 384:512].T[0:1, :]
    gates[4:8, :] = jnp.zeros((4, 256), F32)
    spots = lax.broadcasted_iota(jnp.int32, (1, 4), 1)
    held = jnp.sum(jnp.where(spots == z, bias[...], 0.0), axis=1, keepdims=True)
    v = gates[...] + held + math.log(seq_len)
    u = jnp.exp(-jnp.abs(v))
    w1 = 1.0 + u
    soft = jnp.where(w1 == 1.0, u, jnp.log(w1) * (u / jnp.where(w1 == 1.0, 1.0, w1 - 1.0)))
    logs = jnp.minimum(v, 0.0) - soft
    upper = (
        lax.broadcasted_iota(jnp.int32, (256, 256), 0)
        <= lax.broadcasted_iota(jnp.int32, (256, 256), 1)
    ).astype(BF)
    total = jnp.zeros((8, 256), F32)
    for piece in in_parts(logs):
        total = total + jnp.dot(piece, upper, preferred_element_type=F32)
    pieces = in_parts(total)
    cum_out[0:16, :] = jnp.concatenate([pieces[0].astype(F32), pieces[1].astype(F32)]).astype(BF)
    cum_out[16:32, :] = jnp.concatenate(
        [pieces[2].astype(F32), jnp.zeros((8, 256), F32)]
    ).astype(BF)


def in_parts(value):
    high = value.astype(BF)
    rest = value - high.astype(F32)
    middle = rest.astype(BF)
    low = (rest - middle.astype(F32)).astype(BF)
    return high, middle, low


def attend_body(slots, first, last, scale, at, q, *refs):
    n = len(slots)
    cums, refs = refs[:5], refs[5:]
    kvs, refs = refs[:n], refs[n:]
    if first:
        m_in = acc_in = None
    else:
        m_in, acc_in = refs[:2]
        refs = refs[2:]
    if last:
        chunks = refs[:4]
        refs = refs[4:]
    else:
        m_out, acc_out = refs[:2]
        refs = refs[2:]
    k_all, v_all, scores, probs = refs
    y, c = at[1], at[2]
    place = {}
    local = {}
    for s, (ref, start) in CUM_AT.items():
        got = cums[ref][start : start + 32, :].astype(F32)
        local[s] = got[0:8] + got[8:16] + got[16:24]
        core = c if s[0] else 1 - c
        place[s] = near(y, core, s[1]) * 2 + core
    ends = {s: local[s][:, 255:256] for s in local}
    row = lax.broadcasted_iota(jnp.int32, (8, 1), 0)
    every = functools.reduce(jnp.add, ends.values())
    before = jnp.zeros((8, 1), F32)
    for i in range(3):
        before = before + jnp.where(row > i, every[i : i + 1, :], 0.0)

    def absolute(s):
        inner = before
        for t in ends:
            inner = inner + jnp.where(place[t] < place[s], ends[t], 0.0)
        return (local[s] + inner) * LOG2E

    here = place[True, 0]
    own_cum = absolute((True, 0))
    bias_full, bias_edge = [], []
    for s in slots:
        b = own_cum if s == (True, 0) else absolute(s)
        bias_full.append(b)
        bias_edge.append(b if s == (True, 0) else jnp.where(place[s] < here, b, -NEG))
    ones = jnp.ones((256, 128), BF)
    for zk in range(4):
        for i in range(n):
            block = slice((zk * n + i) * 256, (zk * n + i + 1) * 256)
            k_all[block, :] = kvs[i][zk * 256 : (zk + 1) * 256, 0:128]
            v_all[block, 0:128] = kvs[i][zk * 256 : (zk + 1) * 256, 128:256]
            v_all[block, 128:256] = ones
    causal = lax.broadcasted_iota(jnp.int32, (256, 256), 1) <= lax.broadcasted_iota(
        jnp.int32, (256, 256), 0
    )
    for zq in range(4):
        rows = slice(zq * 256, (zq + 1) * 256)
        queries = q[rows, :]
        cum_t = jnp.broadcast_to(own_cum[zq : zq + 1, :], (128, 256)).T
        top = jnp.full((256, 128), NEG, F32)
        for zk in range(zq + 1):
            for i in range(n):
                block = slice((zk * n + i) * 256, (zk * n + i + 1) * 256)
                bias = (bias_edge if zk == zq else bias_full)[i][zk : zk + 1, :]
                got = (
                    lax.dot_general(
                        queries, k_all[block, :], (((1,), (1,)), ((), ())),
                        preferred_element_type=F32,
                    )
                    * (scale * LOG2E)
                    - bias
                )
                if zk == zq and slots[i] == (True, 0):
                    got = jnp.where(causal, got, NEG)
                scores[:, block] = got
                top = jnp.maximum(top, jnp.maximum(got[:, 0:128], got[:, 128:256]))
        peak = jnp.broadcast_to(jnp.max(top, axis=1, keepdims=True), (256, 128)) + cum_t
        if not first:
            old = m_in[rows, :]
            peak = jnp.maximum(peak, old)
        shift = cum_t - peak
        shift = jnp.concatenate([shift, shift], axis=1)
        for b in range((zq + 1) * n):
            block = slice(b * 256, (b + 1) * 256)
            probs[:, block] = jnp.exp2(scores[:, block] + shift).astype(BF)
        width = (zq + 1) * n * 256
        acc = jnp.dot(probs[:, 0:width], v_all[0:width, :], preferred_element_type=F32)
        if not first:
            factor = jnp.exp2(old - peak)
            acc = acc + acc_in[rows, :] * jnp.concatenate([factor, factor], axis=1)
        if last:
            done = (acc[:, 0:128] / acc[:, 128:256]).astype(BF)
            for s in range(4):

                @pl.when(lax.rem(at[0] + s, 4) == zq)
                def _(s=s, done=done):
                    chunks[s][...] = done

        else:
            m_out[rows, :] = peak
            acc_out[rows, :] = acc


def emit_body(at, *refs):
    att = refs[0:4]
    own_w, other_w = refs[4:8], refs[8:12]
    outs = refs[12:16]
    joined, weights, whole = refs[16:]
    z, y, c, x = at[0], at[1], at[2], at[3]
    for s in range(4):
        zs = slot_of(z, s, 4)
        joined[:, pl.ds(pl.multiple_of(zs * 128, 128), 128)] = att[s][...]
        for j in range(4):
            for k, w in ((c, own_w[j]), (1 - c, other_w[j])):
                ys = near(y, k, j)
                place = pl.ds(pl.multiple_of((zs * 8 + ys * 2 + k) * 32, 32), 32)
                weights[place, :] = w[s * 64 + 32 : s * 64 + 64, :]
    whole[...] = lax.dot_general(
        joined[...], weights[...], (((1,), (1,)), ((), ())), preferred_element_type=F32
    )
    for s in range(4):
        xs = lax.rem(x + s, 4)
        got = whole[pl.ds(pl.multiple_of(xs * 64, 64), 64), :]
        outs[s][...] = got.astype(outs[s].dtype)


def finish_body(at, own, r1, r2, r3, gain, out):
    total = own[...] + r1[...].astype(F32) + r2[...].astype(F32) + r3[...].astype(F32)
    mean = jnp.mean(total * total, axis=1, keepdims=True)
    out[...] = (total * lax.rsqrt(mean + 1e-06) * gain[...]).astype(BF)


def shape(*dims, dtype=BF):
    return jax.ShapeDtypeStruct(dims, dtype)


TURN = (2, 1, 3)


def ring(axis, values):
    got = [values[0], None, None, None]
    for s in TURN:
        got[s] = around(axis, s, values[s], 4)
    return got


CUM_AT = {
    (True, 0): (0, 0),
    (False, 0): (1, 0),
    (True, 1): (2, 0),
    (False, 2): (2, 32),
    (False, 1): (3, 0),
    (True, 2): (3, 32),
    (True, 3): (4, 0),
    (False, 3): (4, 32),
}
GROUPS = (
    ((True, 0), (False, 0)),
    ((True, 2), (False, 2)),
    ((True, 1), (True, 3)),
    ((False, 1), (False, 3)),
)


def layer(tokens, wq, wk, wv, gate, forget_bias, out_weight, out_gain):
    z, y = lax.axis_index("z"), lax.axis_index("y")
    c, x = lax.axis_index("c"), lax.axis_index("x")
    at = jnp.stack([z, y, c, x]).astype(jnp.int32)
    bias = forget_bias.reshape(1, 4)
    seq_len = tokens.shape[0] * 128

    *first, a_own = named(pack_body, [shape(128, 512)] * 4 + [shape(64, 512)], first=True)(
        at, tokens, wq, wk, wv, gate.T, out_weight.T
    )
    a_x = spread("x", a_own)
    by_z = ring("z", first)

    mine = jnp.concatenate([m[64:128] for m in by_z], axis=0)
    own_w = spread("y", mine)
    b_half = spread("x", jnp.concatenate([m[0:64] for m in by_z], axis=0))
    a_half = spread("z", jnp.concatenate(a_x, axis=0))
    other_w = [around("c", 1, w, 2) for w in own_w]

    q, kv, cum = named(
        functools.partial(project_body, seq_len),
        [shape(1024, 128), shape(1024, 256), shape(32, 256)],
        [
            pltpu.VMEM((1024, 1024), BF),
            pltpu.VMEM((1024, 512), BF),
            pltpu.VMEM((8, 256), F32),
        ],
    )(at, bias, *a_half, *b_half, *own_w, *other_w)

    cum_mate = around("c", 1, cum, 2)
    cum_near = along("y", 1, jnp.concatenate([cum, cum_mate], axis=0))
    cum_far = along("y", 1, cum_near)
    cums = [cum, cum_mate, cum_near, around("c", 1, cum_near, 2), cum_far]
    kv_own = spread("y", kv, step=-1)
    where = {(True, j): kv_own[j] for j in range(4)}
    where |= {(False, j): around("c", 1, kv_own[j], 2) for j in range(4)}

    state = ()
    for g, slots in enumerate(GROUPS):
        n = len(slots)
        first_call, last_call = g == 0, g == len(GROUPS) - 1
        outs = (
            [shape(256, 128)] * 4
            if last_call
            else [shape(1024, 128, dtype=F32), shape(1024, 256, dtype=F32)]
        )
        state = named(
            functools.partial(attend_body, slots, first_call, last_call, 128 ** -0.5),
            outs,
            [
                pltpu.VMEM((n * 1024, 128), BF),
                pltpu.VMEM((n * 1024, 256), BF),
                pltpu.VMEM((256, n * 1024), F32),
                pltpu.VMEM((256, n * 1024), BF),
            ],
        )(at, q, *cums, *[where[s] for s in slots], *state)

    att = ring("z", state)
    own, *rest = named(
        emit_body,
        [shape(64, 1024, dtype=F32)] + [shape(64, 1024)] * 3,
        [
            pltpu.VMEM((256, 512), BF),
            pltpu.VMEM((1024, 512), BF),
            pltpu.VMEM((256, 1024), F32),
        ],
    )(at, *att, *own_w, *other_w)
    got = ring("x", [own, *rest])
    (out,) = named(finish_body, [shape(64, 1024)], last=True)(at, *got, out_gain.reshape(1, 1024))
    return out


def solution(mesh):
    torus = Mesh(mesh.devices.reshape(4, 4, 2, 4), ("z", "y", "c", "x"))
    sp = ("z", "y", "c")
    in_specs = (
        P(sp + ("x",), None),
        P(sp, "x"),
        P(sp, "x"),
        P(sp, "x"),
        P(sp, "x"),
        P("x"),
        P("x", sp),
        P(),
    )
    return jax.shard_map(
        layer, mesh=torus, in_specs=in_specs, out_specs=P(sp + ("x",), None), check_vma=False
    )
```

```python
import functools
import math

import jax
import jax.numpy as jnp
from jax import lax
from jax.experimental import pallas as pl
from jax.experimental.pallas import tpu as pltpu
from jax.sharding import Mesh
from jax.sharding import PartitionSpec as P


BF = jnp.bfloat16
F32 = jnp.float32
LOG2E = math.log2(math.e)
NEG = -1e30
VMEM = pl.BlockSpec(memory_space=pltpu.VMEM)
SMEM = pl.BlockSpec(memory_space=pltpu.SMEM)


def named(body, outs, scratch=(), mib=20, first=False, last=False):
    space = pltpu.HBM if first else pltpu.VMEM

    def run(at, *operands):
        return pl.pallas_call(
            body,
            out_shape=outs if last else [pltpu.VMEM(o.shape, o.dtype) for o in outs],
            in_specs=[SMEM] + [VMEM] * len(operands),
            out_specs=[VMEM] * len(outs),
            scratch_shapes=list(scratch),
            compiler_params=pltpu.CompilerParams(vmem_limit_bytes=mib * 1024 * 1024),
        )(at, *(pltpu.with_memory_space_constraint(o, space) for o in operands))

    return run


def around(axis, shift, value, size):
    return lax.ppermute(value, axis, [(i, (i + shift) % size) for i in range(size)])


def along(axis, step, value):
    names, index = ((axis, "c"), lambda i, c: 2 * (i % 4) + c)
    if axis == "x":
        names, index = (("c", "x"), lambda i, c: 4 * c + i % 4)
    pairs = [
        (index(i, c), index(i + (step, -step)[c], c)) for i in range(4) for c in range(2)
    ]
    return lax.ppermute(value, names, pairs)


def spread(axis, value, step=1):
    first = along(axis, step, value)
    second = along(axis, -step, value)
    pair = [first, second] if step == 1 else [second, first]
    return [value, *pair, along(axis, step, first)]


def near(index, core, slot):
    return lax.rem(index + (0, 3 + 2 * core, 1 + 2 * core, 2)[slot], 4)


def slot_of(index, shift, size):
    return lax.rem(index + (size - shift), size)


def pack_body(at, tok, wq, wk, wv, gate, ow, *outs):
    z = at[0]
    row4 = lax.broadcasted_iota(jnp.int32, (4, 32), 0)
    lane = lax.broadcasted_iota(jnp.int32, (32, 128), 1)
    gates = gate[...].astype(F32)
    for s in range(4):
        head = lax.rem(z + s, 4)
        o = outs[s]
        o[0:64, :] = tok[:, 512:1024]
        take = pl.ds(pl.multiple_of(head * 128, 128), 128)
        o[64:96, 0:128] = wq[:, take]
        o[64:96, 128:256] = wk[:, take]
        o[64:96, 256:384] = wv[:, take]
        line = jnp.sum(jnp.where(row4 == head, gates, 0.0), axis=0, keepdims=True)
        column = jnp.broadcast_to(line, (128, 32)).T
        o[64:96, 384:512] = jnp.where(lane == 0, column, 0.0).astype(BF)
        o[96:128, :] = ow[...]
    outs[4][...] = tok[:, 0:512]


def project_body(seq_len, at, *refs):
    bias, refs = refs[0], refs[1:]
    a_half, b_half = refs[0:4], refs[4:8]
    own_w, other_w = refs[8:12], refs[12:16]
    q_out, kv_out, cum_out = refs[16:19]
    toks, weights, gates = refs[19:]
    z, y, c, x = at[0], at[1], at[2], at[3]
    for s in range(4):
        zs = slot_of(z, s, 4)
        zn = near(z, c, s)
        for i in range(4):
            xs = near(x, c, i)
            place = pl.ds(pl.multiple_of((zn * 4 + xs) * 64, 64), 64)
            toks[place, 0:512] = a_half[s][i * 64 : (i + 1) * 64, :]
            place = pl.ds(pl.multiple_of((zs * 4 + xs) * 64, 64), 64)
            toks[place, 512:1024] = b_half[i][s * 64 : (s + 1) * 64, :]
        for j in range(4):
            for k, w in ((c, own_w[j]), (1 - c, other_w[j])):
                ys = near(y, k, j)
                place = pl.ds(pl.multiple_of((zs * 8 + ys * 2 + k) * 32, 32), 32)
                weights[place, :] = w[s * 64 : s * 64 + 32, :]
    whole = weights[...]
    for r in range(4):
        part = slice(r * 256, (r + 1) * 256)
        got = jnp.dot(toks[part, :], whole, preferred_element_type=F32)
        q_out[part, :] = got[:, 0:128].astype(BF)
        kv_out[part, :] = got[:, 128:384].astype(BF)
        gates[r : r + 1, :] = got[:, 384:512].T[0:1, :]
    gates[4:8, :] = jnp.zeros((4, 256), F32)
    spots = lax.broadcasted_iota(jnp.int32, (1, 4), 1)
    held = jnp.sum(jnp.where(spots == z, bias[...], 0.0), axis=1, keepdims=True)
    v = gates[...] + held + math.log(seq_len)
    u = jnp.exp(-jnp.abs(v))
    w1 = 1.0 + u
    soft = jnp.where(w1 == 1.0, u, jnp.log(w1) * (u / jnp.where(w1 == 1.0, 1.0, w1 - 1.0)))
    logs = jnp.minimum(v, 0.0) - soft
    upper = (
        lax.broadcasted_iota(jnp.int32, (256, 256), 0)
        <= lax.broadcasted_iota(jnp.int32, (256, 256), 1)
    ).astype(BF)
    total = jnp.zeros((8, 256), F32)
    for piece in in_parts(logs):
        total = total + jnp.dot(piece, upper, preferred_element_type=F32)
    pieces = in_parts(total)
    cum_out[0:16, :] = jnp.concatenate([pieces[0].astype(F32), pieces[1].astype(F32)]).astype(BF)
    cum_out[16:32, :] = jnp.concatenate(
        [pieces[2].astype(F32), jnp.zeros((8, 256), F32)]
    ).astype(BF)


def in_parts(value):
    high = value.astype(BF)
    rest = value - high.astype(F32)
    middle = rest.astype(BF)
    low = (rest - middle.astype(F32)).astype(BF)
    return high, middle, low


def attend_body(slots, first, last, scale, at, q, *refs):
    n = len(slots)
    cums, refs = refs[:5], refs[5:]
    kvs, refs = refs[:n], refs[n:]
    if first:
        m_in = acc_in = None
    else:
        m_in, acc_in = refs[:2]
        refs = refs[2:]
    if last:
        chunks = refs[:4]
        refs = refs[4:]
    else:
        m_out, acc_out = refs[:2]
        refs = refs[2:]
    k_all, v_all, scores, probs, whole = refs
    y, c = at[1], at[2]
    place = {}
    local = {}
    for s, (ref, start) in CUM_AT.items():
        got = cums[ref][start : start + 32, :].astype(F32)
        local[s] = got[0:8] + got[8:16] + got[16:24]
        core = c if s[0] else 1 - c
        place[s] = near(y, core, s[1]) * 2 + core
    ends = {s: local[s][:, 255:256] for s in local}
    row = lax.broadcasted_iota(jnp.int32, (8, 1), 0)
    every = functools.reduce(jnp.add, ends.values())
    before = jnp.zeros((8, 1), F32)
    for i in range(3):
        before = before + jnp.where(row > i, every[i : i + 1, :], 0.0)

    def absolute(s):
        inner = before
        for t in ends:
            inner = inner + jnp.where(place[t] < place[s], ends[t], 0.0)
        return (local[s] + inner) * LOG2E

    here = place[True, 0]
    own_cum = absolute((True, 0))
    bias_full, bias_edge = [], []
    for s in slots:
        b = own_cum if s == (True, 0) else absolute(s)
        bias_full.append(b)
        bias_edge.append(b if s == (True, 0) else jnp.where(place[s] < here, b, -NEG))
    ones = jnp.ones((256, 128), BF)
    for zk in range(4):
        for i in range(n):
            block = slice((zk * n + i) * 256, (zk * n + i + 1) * 256)
            k_all[block, :] = kvs[i][zk * 256 : (zk + 1) * 256, 0:128]
            v_all[block, 0:128] = kvs[i][zk * 256 : (zk + 1) * 256, 128:256]
            v_all[block, 128:256] = ones
    causal = lax.broadcasted_iota(jnp.int32, (256, 256), 1) <= lax.broadcasted_iota(
        jnp.int32, (256, 256), 0
    )
    for zq in range(4):
        rows = slice(zq * 256, (zq + 1) * 256)
        queries = q[rows, :]
        cum_t = jnp.broadcast_to(own_cum[zq : zq + 1, :], (128, 256)).T
        top = jnp.full((256, 128), NEG, F32)
        for zk in range(zq + 1):
            for i in range(n):
                block = slice((zk * n + i) * 256, (zk * n + i + 1) * 256)
                bias = (bias_edge if zk == zq else bias_full)[i][zk : zk + 1, :]
                got = (
                    lax.dot_general(
                        queries, k_all[block, :], (((1,), (1,)), ((), ())),
                        preferred_element_type=F32,
                    )
                    * (scale * LOG2E)
                    - bias
                )
                if zk == zq and slots[i] == (True, 0):
                    got = jnp.where(causal, got, NEG)
                scores[:, block] = got
                top = jnp.maximum(top, jnp.maximum(got[:, 0:128], got[:, 128:256]))
        peak = jnp.broadcast_to(jnp.max(top, axis=1, keepdims=True), (256, 128)) + cum_t
        if not first:
            old = m_in[rows, :]
            peak = jnp.maximum(peak, old)
        shift = cum_t - peak
        shift = jnp.concatenate([shift, shift], axis=1)
        for b in range((zq + 1) * n):
            block = slice(b * 256, (b + 1) * 256)
            probs[:, block] = jnp.exp2(scores[:, block] + shift).astype(BF)
        width = (zq + 1) * n * 256
        acc = jnp.dot(probs[:, 0:width], v_all[0:width, :], preferred_element_type=F32)
        if not first:
            factor = jnp.exp2(old - peak)
            acc = acc + acc_in[rows, :] * jnp.concatenate([factor, factor], axis=1)
        if last:
            whole[rows, :] = (acc[:, 0:128] / acc[:, 128:256]).astype(BF)
        else:
            m_out[rows, :] = peak
            acc_out[rows, :] = acc
    if last:
        for s in range(4):
            zs = lax.rem(at[0] + s, 4)
            chunks[s][...] = whole[pl.ds(pl.multiple_of(zs * 256, 256), 256), :]


def emit_body(at, *refs):
    att = refs[0:4]
    own_w, other_w = refs[4:8], refs[8:12]
    outs = refs[12:16]
    joined, weights, whole = refs[16:]
    z, y, c, x = at[0], at[1], at[2], at[3]
    for s in range(4):
        zs = slot_of(z, s, 4)
        joined[:, pl.ds(pl.multiple_of(zs * 128, 128), 128)] = att[s][...]
        for j in range(4):
            for k, w in ((c, own_w[j]), (1 - c, other_w[j])):
                ys = near(y, k, j)
                place = pl.ds(pl.multiple_of((zs * 8 + ys * 2 + k) * 32, 32), 32)
                weights[place, :] = w[s * 64 + 32 : s * 64 + 64, :]
    whole[...] = lax.dot_general(
        joined[...], weights[...], (((1,), (1,)), ((), ())), preferred_element_type=F32
    )
    for s in range(4):
        xs = lax.rem(x + s, 4)
        got = whole[pl.ds(pl.multiple_of(xs * 64, 64), 64), :]
        outs[s][...] = got.astype(outs[s].dtype)


def finish_body(at, own, r1, r2, r3, gain, out):
    total = own[...] + r1[...].astype(F32) + r2[...].astype(F32) + r3[...].astype(F32)
    mean = jnp.mean(total * total, axis=1, keepdims=True)
    out[...] = (total * lax.rsqrt(mean + 1e-06) * gain[...]).astype(BF)


def shape(*dims, dtype=BF):
    return jax.ShapeDtypeStruct(dims, dtype)


TURN = (2, 1, 3)


def ring(axis, values):
    got = [values[0], None, None, None]
    for s in TURN:
        got[s] = around(axis, s, values[s], 4)
    return got


CUM_AT = {
    (True, 0): (0, 0),
    (False, 0): (1, 0),
    (True, 1): (2, 0),
    (False, 2): (2, 32),
    (False, 1): (3, 0),
    (True, 2): (3, 32),
    (True, 3): (4, 0),
    (False, 3): (4, 32),
}
GROUPS = (
    ((True, 0), (False, 0)),
    ((True, 2), (False, 2)),
    ((True, 1), (True, 3)),
    ((False, 1), (False, 3)),
)


def layer(tokens, wq, wk, wv, gate, forget_bias, out_weight, out_gain):
    z, y = lax.axis_index("z"), lax.axis_index("y")
    c, x = lax.axis_index("c"), lax.axis_index("x")
    at = jnp.stack([z, y, c, x]).astype(jnp.int32)
    bias = forget_bias.reshape(1, 4)
    seq_len = tokens.shape[0] * 128

    *first, a_own = named(pack_body, [shape(128, 512)] * 4 + [shape(64, 512)], first=True)(
        at, tokens, wq, wk, wv, gate.T, out_weight.T
    )
    a_x = spread("x", a_own)
    by_z = ring("z", first)

    mine = jnp.concatenate([m[64:128] for m in by_z], axis=0)
    own_w = spread("y", mine)
    b_half = spread("x", jnp.concatenate([m[0:64] for m in by_z], axis=0))
    a_half = spread("z", jnp.concatenate(a_x, axis=0))
    other_w = [around("c", 1, w, 2) for w in own_w]

    q, kv, cum = named(
        functools.partial(project_body, seq_len),
        [shape(1024, 128), shape(1024, 256), shape(32, 256)],
        [
            pltpu.VMEM((1024, 1024), BF),
            pltpu.VMEM((1024, 512), BF),
            pltpu.VMEM((8, 256), F32),
        ],
    )(at, bias, *a_half, *b_half, *own_w, *other_w)

    cum_mate = around("c", 1, cum, 2)
    cum_near = along("y", 1, jnp.concatenate([cum, cum_mate], axis=0))
    cum_far = along("y", 1, cum_near)
    cums = [cum, cum_mate, cum_near, around("c", 1, cum_near, 2), cum_far]
    kv_own = spread("y", kv, step=-1)
    where = {(True, j): kv_own[j] for j in range(4)}
    where |= {(False, j): around("c", 1, kv_own[j], 2) for j in range(4)}

    state = ()
    for g, slots in enumerate(GROUPS):
        n = len(slots)
        first_call, last_call = g == 0, g == len(GROUPS) - 1
        outs = (
            [shape(256, 128)] * 4
            if last_call
            else [shape(1024, 128, dtype=F32), shape(1024, 256, dtype=F32)]
        )
        state = named(
            functools.partial(attend_body, slots, first_call, last_call, 128 ** -0.5),
            outs,
            [
                pltpu.VMEM((n * 1024, 128), BF),
                pltpu.VMEM((n * 1024, 256), BF),
                pltpu.VMEM((256, n * 1024), F32),
                pltpu.VMEM((256, n * 1024), BF),
                pltpu.VMEM((1024, 128), BF),
            ],
        )(at, q, *cums, *[where[s] for s in slots], *state)

    att = ring("z", state)
    own, *rest = named(
        emit_body,
        [shape(64, 1024, dtype=F32)] + [shape(64, 1024)] * 3,
        [
            pltpu.VMEM((256, 512), BF),
            pltpu.VMEM((1024, 512), BF),
            pltpu.VMEM((256, 1024), F32),
        ],
    )(at, *att, *own_w, *other_w)
    got = ring("x", [own, *rest])
    (out,) = named(finish_body, [shape(64, 1024)], last=True)(
        at, *got, out_gain.reshape(1, 1024)
    )
    return out


def solution(mesh):
    torus = Mesh(mesh.devices.reshape(4, 4, 2, 4), ("z", "y", "c", "x"))
    sp = ("z", "y", "c")
    in_specs = (
        P(sp + ("x",), None),
        P(sp, "x"),
        P(sp, "x"),
        P(sp, "x"),
        P(sp, "x"),
        P("x"),
        P("x", sp),
        P(),
    )
    return jax.shard_map(
        layer, mesh=torus, in_specs=in_specs, out_specs=P(sp + ("x",), None), check_vma=False
    )
```

```python
import functools
import math

import jax
import jax.numpy as jnp
from jax import lax
from jax.experimental import pallas as pl
from jax.experimental.pallas import tpu as pltpu
from jax.sharding import Mesh
from jax.sharding import PartitionSpec as P


BF = jnp.bfloat16
F32 = jnp.float32
LOG2E = math.log2(math.e)
NEG = -1e30
VMEM = pl.BlockSpec(memory_space=pltpu.VMEM)
SMEM = pl.BlockSpec(memory_space=pltpu.SMEM)


def named(body, outs, scratch=(), mib=20, first=False, last=False):
    space = pltpu.HBM if first else pltpu.VMEM

    def run(at, *operands):
        return pl.pallas_call(
            body,
            out_shape=outs if last else [pltpu.VMEM(o.shape, o.dtype) for o in outs],
            in_specs=[SMEM] + [VMEM] * len(operands),
            out_specs=[VMEM] * len(outs),
            scratch_shapes=list(scratch),
            compiler_params=pltpu.CompilerParams(vmem_limit_bytes=mib * 1024 * 1024),
        )(at, *(pltpu.with_memory_space_constraint(o, space) for o in operands))

    return run


def around(axis, shift, value, size):
    return lax.ppermute(value, axis, [(i, (i + shift) % size) for i in range(size)])


def along(axis, step, value):
    names, index = ((axis, "c"), lambda i, c: 2 * (i % 4) + c)
    if axis == "x":
        names, index = (("c", "x"), lambda i, c: 4 * c + i % 4)
    pairs = [
        (index(i, c), index(i + (step, -step)[c], c)) for i in range(4) for c in range(2)
    ]
    return lax.ppermute(value, names, pairs)


def spread(axis, value, step=1):
    first = along(axis, step, value)
    second = along(axis, -step, value)
    pair = [first, second] if step == 1 else [second, first]
    return [value, *pair, along(axis, step, first)]


def near(index, core, slot):
    return lax.rem(index + (0, 3 + 2 * core, 1 + 2 * core, 2)[slot], 4)


def slot_of(index, shift, size):
    return lax.rem(index + (size - shift), size)


def pack_body(at, tok, wq, wk, wv, gate, ow, *outs):
    z = at[0]
    row4 = lax.broadcasted_iota(jnp.int32, (4, 32), 0)
    lane = lax.broadcasted_iota(jnp.int32, (32, 128), 1)
    gates = gate[...].astype(F32)
    for s in range(4):
        head = lax.rem(z + s, 4)
        o = outs[s]
        o[0:64, :] = tok[:, 512:1024]
        take = pl.ds(pl.multiple_of(head * 128, 128), 128)
        o[64:96, 0:128] = wq[:, take]
        o[64:96, 128:256] = wk[:, take]
        o[64:96, 256:384] = wv[:, take]
        line = jnp.sum(jnp.where(row4 == head, gates, 0.0), axis=0, keepdims=True)
        column = jnp.broadcast_to(line, (128, 32)).T
        o[64:96, 384:512] = jnp.where(lane == 0, column, 0.0).astype(BF)
        o[96:128, :] = ow[...]
    outs[4][...] = tok[:, 0:512]


def project_body(seq_len, at, *refs):
    bias, refs = refs[0], refs[1:]
    a_half, b_half = refs[0:4], refs[4:8]
    own_w, other_w = refs[8:12], refs[12:16]
    q_out, kv_out, cum_out = refs[16:19]
    toks, weights, gates = refs[19:]
    z, y, c, x = at[0], at[1], at[2], at[3]
    for s in range(4):
        zs = slot_of(z, s, 4)
        zn = near(z, c, s)
        for i in range(4):
            xs = near(x, c, i)
            place = pl.ds(pl.multiple_of((zn * 4 + xs) * 64, 64), 64)
            toks[place, 0:512] = a_half[s][i * 64 : (i + 1) * 64, :]
            place = pl.ds(pl.multiple_of((zs * 4 + xs) * 64, 64), 64)
            toks[place, 512:1024] = b_half[i][s * 64 : (s + 1) * 64, :]
        for j in range(4):
            for k, w in ((c, own_w[j]), (1 - c, other_w[j])):
                ys = near(y, k, j)
                place = pl.ds(pl.multiple_of((zs * 8 + ys * 2 + k) * 32, 32), 32)
                weights[place, :] = w[s * 64 : s * 64 + 32, :]
    whole = weights[...]
    for r in range(4):
        part = slice(r * 256, (r + 1) * 256)
        got = jnp.dot(toks[part, :], whole, preferred_element_type=F32)
        q_out[part, :] = got[:, 0:128].astype(BF)
        kv_out[part, :] = got[:, 128:384].astype(BF)
        gates[r : r + 1, :] = got[:, 384:512].T[0:1, :]
    gates[4:8, :] = jnp.zeros((4, 256), F32)
    spots = lax.broadcasted_iota(jnp.int32, (1, 4), 1)
    held = jnp.sum(jnp.where(spots == z, bias[...], 0.0), axis=1, keepdims=True)
    v = gates[...] + held + math.log(seq_len)
    u = jnp.exp(-jnp.abs(v))
    w1 = 1.0 + u
    soft = jnp.where(w1 == 1.0, u, jnp.log(w1) * (u / jnp.where(w1 == 1.0, 1.0, w1 - 1.0)))
    logs = jnp.minimum(v, 0.0) - soft
    upper = (
        lax.broadcasted_iota(jnp.int32, (256, 256), 0)
        <= lax.broadcasted_iota(jnp.int32, (256, 256), 1)
    ).astype(BF)
    total = jnp.zeros((8, 256), F32)
    for piece in in_parts(logs):
        total = total + jnp.dot(piece, upper, preferred_element_type=F32)
    pieces = in_parts(total)
    cum_out[0:16, :] = jnp.concatenate([pieces[0].astype(F32), pieces[1].astype(F32)]).astype(BF)
    cum_out[16:32, :] = jnp.concatenate(
        [pieces[2].astype(F32), jnp.zeros((8, 256), F32)]
    ).astype(BF)


def in_parts(value):
    high = value.astype(BF)
    rest = value - high.astype(F32)
    middle = rest.astype(BF)
    low = (rest - middle.astype(F32)).astype(BF)
    return high, middle, low


def attend_body(slots, first, last, scale, at, q, *refs):
    n = len(slots)
    cums, refs = refs[:5], refs[5:]
    kvs, refs = refs[:n], refs[n:]
    if first:
        m_in = acc_in = None
    else:
        m_in, acc_in = refs[:2]
        refs = refs[2:]
    if last:
        chunks = refs[:4]
        refs = refs[4:]
    else:
        m_out, acc_out = refs[:2]
        refs = refs[2:]
    v_all, scores, probs, whole = refs
    y, c = at[1], at[2]
    place = {}
    local = {}
    for s, (ref, start) in CUM_AT.items():
        got = cums[ref][start : start + 32, :].astype(F32)
        local[s] = got[0:8] + got[8:16] + got[16:24]
        core = c if s[0] else 1 - c
        place[s] = near(y, core, s[1]) * 2 + core
    ends = {s: local[s][:, 255:256] for s in local}
    row = lax.broadcasted_iota(jnp.int32, (8, 1), 0)
    every = functools.reduce(jnp.add, ends.values())
    before = jnp.zeros((8, 1), F32)
    for i in range(3):
        before = before + jnp.where(row > i, every[i : i + 1, :], 0.0)

    def absolute(s):
        inner = before
        for t in ends:
            inner = inner + jnp.where(place[t] < place[s], ends[t], 0.0)
        return (local[s] + inner) * LOG2E

    here = place[True, 0]
    own_cum = absolute((True, 0))
    bias_full, bias_edge = [], []
    for s in slots:
        b = own_cum if s == (True, 0) else absolute(s)
        bias_full.append(b)
        bias_edge.append(b if s == (True, 0) else jnp.where(place[s] < here, b, -NEG))
    ones = jnp.ones((256, 128), BF)
    for zk in range(4):
        for i in range(n):
            block = slice((zk * n + i) * 256, (zk * n + i + 1) * 256)
            v_all[block, 0:128] = kvs[i][zk * 256 : (zk + 1) * 256, 128:256]
            v_all[block, 128:256] = ones
    causal = lax.broadcasted_iota(jnp.int32, (256, 256), 1) <= lax.broadcasted_iota(
        jnp.int32, (256, 256), 0
    )
    begin = {3: 0, 2: 4 * n, 1: 7 * n, 0: 9 * n}
    shifts, keep = {}, {}

    def score(zq):
        rows = slice(zq * 256, (zq + 1) * 256)
        queries = q[rows, :]
        cum_t = jnp.broadcast_to(own_cum[zq : zq + 1, :], (128, 256)).T
        top = jnp.full((256, 128), NEG, F32)
        for zk in range(zq + 1):
            for i in range(n):
                b = begin[zq] + zk * n + i
                bias = (bias_edge if zk == zq else bias_full)[i][zk : zk + 1, :]
                got = (
                    lax.dot_general(
                        queries,
                        kvs[i][zk * 256 : (zk + 1) * 256, 0:128],
                        (((1,), (1,)), ((), ())),
                        preferred_element_type=F32,
                    )
                    * (scale * LOG2E)
                    - bias
                )
                if zk == zq and slots[i] == (True, 0):
                    got = jnp.where(causal, got, NEG)
                scores[:, b * 256 : (b + 1) * 256] = got
                top = jnp.maximum(top, jnp.maximum(got[:, 0:128], got[:, 128:256]))
        peak = jnp.broadcast_to(jnp.max(top, axis=1, keepdims=True), (256, 128)) + cum_t
        if not first:
            old = m_in[rows, :]
            peak = jnp.maximum(peak, old)
            keep[zq] = jnp.exp2(old - peak)
        shifts[zq] = cum_t - peak
        if not last:
            m_out[rows, :] = peak

    def weigh(zq):
        shift = jnp.concatenate([shifts[zq], shifts[zq]], axis=1)
        for b in range(begin[zq], begin[zq] + (zq + 1) * n):
            block = slice(b * 256, (b + 1) * 256)
            probs[:, block] = jnp.exp2(scores[:, block] + shift).astype(BF)

    def gather(zq):
        rows = slice(zq * 256, (zq + 1) * 256)
        blocks = (zq + 1) * n
        half = (blocks + 1) // 2
        acc = None
        for lo, hi in ((0, half), (half, blocks)):
            if lo == hi:
                continue
            part = jnp.dot(
                probs[:, (begin[zq] + lo) * 256 : (begin[zq] + hi) * 256],
                v_all[lo * 256 : hi * 256, :],
                preferred_element_type=F32,
            )
            acc = part if acc is None else acc + part
        if not first:
            acc = acc + acc_in[rows, :] * jnp.concatenate([keep[zq], keep[zq]], axis=1)
        if last:
            whole[rows, :] = (acc[:, 0:128] / acc[:, 128:256]).astype(BF)
        else:
            acc_out[rows, :] = acc

    for step in STEPS:
        {"s": score, "w": weigh, "g": gather}[step[0]](int(step[1]))
    if last:
        for s in range(4):
            zs = lax.rem(at[0] + s, 4)
            chunks[s][...] = whole[pl.ds(pl.multiple_of(zs * 256, 256), 256), :]


def emit_body(at, *refs):
    att = refs[0:4]
    own_w, other_w = refs[4:8], refs[8:12]
    outs = refs[12:16]
    joined, weights, whole = refs[16:]
    z, y, c, x = at[0], at[1], at[2], at[3]
    for s in range(4):
        zs = slot_of(z, s, 4)
        joined[:, pl.ds(pl.multiple_of(zs * 128, 128), 128)] = att[s][...]
        for j in range(4):
            for k, w in ((c, own_w[j]), (1 - c, other_w[j])):
                ys = near(y, k, j)
                place = pl.ds(pl.multiple_of((zs * 8 + ys * 2 + k) * 32, 32), 32)
                weights[place, :] = w[s * 64 + 32 : s * 64 + 64, :]
    whole[...] = lax.dot_general(
        joined[...], weights[...], (((1,), (1,)), ((), ())), preferred_element_type=F32
    )
    for s in range(4):
        xs = lax.rem(x + s, 4)
        got = whole[pl.ds(pl.multiple_of(xs * 64, 64), 64), :]
        outs[s][...] = got.astype(outs[s].dtype)


def finish_body(at, own, r1, r2, r3, gain, out):
    total = own[...] + r1[...].astype(F32) + r2[...].astype(F32) + r3[...].astype(F32)
    mean = jnp.mean(total * total, axis=1, keepdims=True)
    out[...] = (total * lax.rsqrt(mean + 1e-06) * gain[...]).astype(BF)


def shape(*dims, dtype=BF):
    return jax.ShapeDtypeStruct(dims, dtype)


TURN = (2, 1, 3)


def ring(axis, values):
    got = [values[0], None, None, None]
    for s in TURN:
        got[s] = around(axis, s, values[s], 4)
    return got


CUM_AT = {
    (True, 0): (0, 0),
    (False, 0): (1, 0),
    (True, 1): (2, 0),
    (False, 2): (2, 32),
    (False, 1): (3, 0),
    (True, 2): (3, 32),
    (True, 3): (4, 0),
    (False, 3): (4, 32),
}
STEPS = ("s3", "s2", "w3", "g3", "s1", "w2", "g2", "s0", "w1", "g1", "w0", "g0")
GROUPS = (
    ((True, 0), (False, 0)),
    ((True, 2), (False, 2)),
    ((True, 1), (True, 3)),
    ((False, 1), (False, 3)),
)


def layer(tokens, wq, wk, wv, gate, forget_bias, out_weight, out_gain):
    z, y = lax.axis_index("z"), lax.axis_index("y")
    c, x = lax.axis_index("c"), lax.axis_index("x")
    at = jnp.stack([z, y, c, x]).astype(jnp.int32)
    bias = forget_bias.reshape(1, 4)
    seq_len = tokens.shape[0] * 128

    *first, a_own = named(pack_body, [shape(128, 512)] * 4 + [shape(64, 512)], first=True)(
        at, tokens, wq, wk, wv, gate.T, out_weight.T
    )
    a_x = spread("x", a_own)
    by_z = ring("z", first)

    mine = jnp.concatenate([m[64:128] for m in by_z], axis=0)
    own_w = spread("y", mine)
    b_half = spread("x", jnp.concatenate([m[0:64] for m in by_z], axis=0))
    a_half = spread("z", jnp.concatenate(a_x, axis=0))
    other_w = [around("c", 1, w, 2) for w in own_w]

    q, kv, cum = named(
        functools.partial(project_body, seq_len),
        [shape(1024, 128), shape(1024, 256), shape(32, 256)],
        [
            pltpu.VMEM((1024, 1024), BF),
            pltpu.VMEM((1024, 512), BF),
            pltpu.VMEM((8, 256), F32),
        ],
    )(at, bias, *a_half, *b_half, *own_w, *other_w)

    cum_mate = around("c", 1, cum, 2)
    cum_pair = jnp.concatenate([cum, cum_mate], axis=0)
    cum_near = along("y", 1, cum_pair)
    cum_far = around("y", 2, cum_pair, 4)
    cums = [cum, cum_mate, cum_near, around("c", 1, cum_near, 2), cum_far]
    kv_own = spread("y", kv, step=-1)
    where = {(True, j): kv_own[j] for j in range(4)}
    where |= {(False, j): around("c", 1, kv_own[j], 2) for j in range(4)}

    state = ()
    for g, slots in enumerate(GROUPS):
        n = len(slots)
        first_call, last_call = g == 0, g == len(GROUPS) - 1
        outs = (
            [shape(256, 128)] * 4
            if last_call
            else [shape(1024, 128, dtype=F32), shape(1024, 256, dtype=F32)]
        )
        state = named(
            functools.partial(attend_body, slots, first_call, last_call, 128 ** -0.5),
            outs,
            [
                pltpu.VMEM((n * 1024, 256), BF),
                pltpu.VMEM((256, n * 2560), F32),
                pltpu.VMEM((256, n * 2560), BF),
                pltpu.VMEM((1024, 128), BF),
            ],
        )(at, q, *cums, *[where[s] for s in slots], *state)

    att = ring("z", state)
    own, *rest = named(
        emit_body,
        [shape(64, 1024, dtype=F32)] + [shape(64, 1024)] * 3,
        [
            pltpu.VMEM((256, 512), BF),
            pltpu.VMEM((1024, 512), BF),
            pltpu.VMEM((256, 1024), F32),
        ],
    )(at, *att, *own_w, *other_w)
    got = ring("x", [own, *rest])
    (out,) = named(finish_body, [shape(64, 1024)], last=True)(
        at, *got, out_gain.reshape(1, 1024)
    )
    return out


def solution(mesh):
    torus = Mesh(mesh.devices.reshape(4, 4, 2, 4), ("z", "y", "c", "x"))
    sp = ("z", "y", "c")
    in_specs = (
        P(sp + ("x",), None),
        P(sp, "x"),
        P(sp, "x"),
        P(sp, "x"),
        P(sp, "x"),
        P("x"),
        P("x", sp),
        P(),
    )
    return jax.shard_map(
        layer, mesh=torus, in_specs=in_specs, out_specs=P(sp + ("x",), None), check_vma=False
    )
```

```python
import functools
import math

import jax
import jax.numpy as jnp
from jax import lax
from jax.experimental import pallas as pl
from jax.experimental.pallas import tpu as pltpu
from jax.sharding import Mesh
from jax.sharding import PartitionSpec as P


BF = jnp.bfloat16
F32 = jnp.float32
LOG2E = math.log2(math.e)
NEG = -1e30
VMEM = pl.BlockSpec(memory_space=pltpu.VMEM)


def named(body, outs, scratch=(), mib=20, first=False, last=False):
    space = pltpu.HBM if first else pltpu.VMEM

    def seated(*refs):
        body([lax.axis_index(axis) for axis in ("z", "y", "c", "x")], *refs)

    def run(*operands):
        return pl.pallas_call(
            seated,
            out_shape=outs if last else [pltpu.VMEM(o.shape, o.dtype) for o in outs],
            in_specs=[VMEM] * len(operands),
            out_specs=[VMEM] * len(outs),
            scratch_shapes=list(scratch),
            compiler_params=pltpu.CompilerParams(vmem_limit_bytes=mib * 1024 * 1024),
        )(*(pltpu.with_memory_space_constraint(o, space) for o in operands))

    return run


def around(axis, shift, value, size):
    return lax.ppermute(value, axis, [(i, (i + shift) % size) for i in range(size)])


def along(axis, step, value):
    names, index = ((axis, "c"), lambda i, c: 2 * (i % 4) + c)
    if axis == "x":
        names, index = (("c", "x"), lambda i, c: 4 * c + i % 4)
    pairs = [
        (index(i, c), index(i + (step, -step)[c], c)) for i in range(4) for c in range(2)
    ]
    return lax.ppermute(value, names, pairs)


def spread(axis, value, step=1):
    first = along(axis, step, value)
    second = along(axis, -step, value)
    pair = [first, second] if step == 1 else [second, first]
    return [value, *pair, along(axis, step, first)]


def near(index, core, slot):
    return lax.rem(index + (0, 3 + 2 * core, 1 + 2 * core, 2)[slot], 4)


def slot_of(index, shift, size):
    return lax.rem(index + (size - shift), size)


def pack_body(at, tok, wq, wk, wv, gate, ow, *outs):
    z = at[0]
    row4 = lax.broadcasted_iota(jnp.int32, (4, 32), 0)
    lane = lax.broadcasted_iota(jnp.int32, (32, 128), 1)
    gates = gate[...].astype(F32)
    for s in range(4):
        head = lax.rem(z + s, 4)
        o = outs[s]
        o[0:64, :] = tok[:, 512:1024]
        take = pl.ds(pl.multiple_of(head * 128, 128), 128)
        o[64:96, 0:128] = wq[:, take]
        o[64:96, 128:256] = wk[:, take]
        o[64:96, 256:384] = wv[:, take]
        line = jnp.sum(jnp.where(row4 == head, gates, 0.0), axis=0, keepdims=True)
        column = jnp.broadcast_to(line, (128, 32)).T
        o[64:96, 384:512] = jnp.where(lane == 0, column, 0.0).astype(BF)
        o[96:128, :] = ow[...]
    outs[4][...] = tok[:, 0:512]


def project_body(seq_len, at, *refs):
    bias, refs = refs[0], refs[1:]
    a_half, b_half = refs[0:4], refs[4:8]
    own_w, other_w = refs[8:12], refs[12:16]
    q_out, kv_out, cum_out = refs[16:19]
    toks, weights, gates = refs[19:]
    z, y, c, x = at[0], at[1], at[2], at[3]
    for s in range(4):
        zs = slot_of(z, s, 4)
        zn = near(z, c, s)
        for i in range(4):
            xs = near(x, c, i)
            place = pl.ds(pl.multiple_of((zn * 4 + xs) * 64, 64), 64)
            toks[place, 0:512] = a_half[s][i * 64 : (i + 1) * 64, :]
            place = pl.ds(pl.multiple_of((zs * 4 + xs) * 64, 64), 64)
            toks[place, 512:1024] = b_half[i][s * 64 : (s + 1) * 64, :]
        for j in range(4):
            for k, w in ((c, own_w[j]), (1 - c, other_w[j])):
                ys = near(y, k, j)
                place = pl.ds(pl.multiple_of((zs * 8 + ys * 2 + k) * 32, 32), 32)
                weights[place, :] = w[s * 64 : s * 64 + 32, :]
    whole = weights[...]
    for r in range(4):
        part = slice(r * 256, (r + 1) * 256)
        got = jnp.dot(toks[part, :], whole, preferred_element_type=F32)
        q_out[part, :] = got[:, 0:128].astype(BF)
        kv_out[part, :] = got[:, 128:384].astype(BF)
        gates[r : r + 1, :] = got[:, 384:512].T[0:1, :]
    gates[4:8, :] = jnp.zeros((4, 256), F32)
    spots = lax.broadcasted_iota(jnp.int32, (1, 4), 1)
    held = jnp.sum(jnp.where(spots == z, bias[...], 0.0), axis=1, keepdims=True)
    v = gates[...] + held + math.log(seq_len)
    u = jnp.exp(-jnp.abs(v))
    w1 = 1.0 + u
    soft = jnp.where(w1 == 1.0, u, jnp.log(w1) * (u / jnp.where(w1 == 1.0, 1.0, w1 - 1.0)))
    logs = jnp.minimum(v, 0.0) - soft
    upper = (
        lax.broadcasted_iota(jnp.int32, (256, 256), 0)
        <= lax.broadcasted_iota(jnp.int32, (256, 256), 1)
    ).astype(BF)
    total = jnp.zeros((8, 256), F32)
    for piece in in_parts(logs):
        total = total + jnp.dot(piece, upper, preferred_element_type=F32)
    pieces = in_parts(total)
    cum_out[0:16, :] = jnp.concatenate([pieces[0].astype(F32), pieces[1].astype(F32)]).astype(BF)
    cum_out[16:32, :] = jnp.concatenate(
        [pieces[2].astype(F32), jnp.zeros((8, 256), F32)]
    ).astype(BF)


def in_parts(value):
    high = value.astype(BF)
    rest = value - high.astype(F32)
    middle = rest.astype(BF)
    low = (rest - middle.astype(F32)).astype(BF)
    return high, middle, low


def attend_body(slots, first, last, scale, at, q, *refs):
    n = len(slots)
    cums, refs = refs[:5], refs[5:]
    kvs, refs = refs[:n], refs[n:]
    if first:
        m_in = acc_in = None
    else:
        m_in, acc_in = refs[:2]
        refs = refs[2:]
    if last:
        chunks = refs[:4]
        refs = refs[4:]
    else:
        m_out, acc_out = refs[:2]
        refs = refs[2:]
    v_all, scores, probs, whole = refs
    y, c = at[1], at[2]
    place = {}
    local = {}
    for s, (ref, start) in CUM_AT.items():
        got = cums[ref][start : start + 32, :].astype(F32)
        local[s] = got[0:8] + got[8:16] + got[16:24]
        core = c if s[0] else 1 - c
        place[s] = near(y, core, s[1]) * 2 + core
    ends = {s: local[s][:, 255:256] for s in local}
    row = lax.broadcasted_iota(jnp.int32, (8, 1), 0)
    every = functools.reduce(jnp.add, ends.values())
    before = jnp.zeros((8, 1), F32)
    for i in range(3):
        before = before + jnp.where(row > i, every[i : i + 1, :], 0.0)

    def absolute(s):
        inner = before
        for t in ends:
            inner = inner + jnp.where(place[t] < place[s], ends[t], 0.0)
        return (local[s] + inner) * LOG2E

    here = place[True, 0]
    own_cum = absolute((True, 0))
    bias_full, bias_edge = [], []
    for s in slots:
        b = own_cum if s == (True, 0) else absolute(s)
        bias_full.append(b)
        bias_edge.append(b if s == (True, 0) else jnp.where(place[s] < here, b, -NEG))
    ones = jnp.ones((256, 128), BF)
    for zk in range(4):
        for i in range(n):
            block = slice((zk * n + i) * 256, (zk * n + i + 1) * 256)
            v_all[block, 0:128] = kvs[i][zk * 256 : (zk + 1) * 256, 128:256]
            v_all[block, 128:256] = ones
    causal = lax.broadcasted_iota(jnp.int32, (256, 256), 1) <= lax.broadcasted_iota(
        jnp.int32, (256, 256), 0
    )
    begin = {3: 0, 2: 4 * n, 1: 7 * n, 0: 9 * n}
    shifts, keep = {}, {}

    def score(zq):
        rows = slice(zq * 256, (zq + 1) * 256)
        queries = q[rows, :]
        cum_t = jnp.broadcast_to(own_cum[zq : zq + 1, :], (128, 256)).T
        top = jnp.full((256, 128), NEG, F32)
        for zk in range(zq + 1):
            for i in range(n):
                b = begin[zq] + zk * n + i
                bias = (bias_edge if zk == zq else bias_full)[i][zk : zk + 1, :]
                got = (
                    lax.dot_general(
                        queries,
                        kvs[i][zk * 256 : (zk + 1) * 256, 0:128],
                        (((1,), (1,)), ((), ())),
                        preferred_element_type=F32,
                    )
                    * (scale * LOG2E)
                    - bias
                )
                if zk == zq and slots[i] == (True, 0):
                    got = jnp.where(causal, got, NEG)
                scores[:, b * 256 : (b + 1) * 256] = got
                top = jnp.maximum(top, jnp.maximum(got[:, 0:128], got[:, 128:256]))
        peak = jnp.broadcast_to(jnp.max(top, axis=1, keepdims=True), (256, 128)) + cum_t
        if not first:
            old = m_in[rows, :]
            peak = jnp.maximum(peak, old)
            keep[zq] = jnp.exp2(old - peak)
        shifts[zq] = cum_t - peak
        if not last:
            m_out[rows, :] = peak

    def weigh(zq):
        shift = jnp.concatenate([shifts[zq], shifts[zq]], axis=1)
        for b in range(begin[zq], begin[zq] + (zq + 1) * n):
            block = slice(b * 256, (b + 1) * 256)
            probs[:, block] = jnp.exp2(scores[:, block] + shift).astype(BF)

    def gather(zq):
        rows = slice(zq * 256, (zq + 1) * 256)
        blocks = (zq + 1) * n
        half = (blocks + 1) // 2
        acc = None
        for lo, hi in ((0, half), (half, blocks)):
            if lo == hi:
                continue
            part = jnp.dot(
                probs[:, (begin[zq] + lo) * 256 : (begin[zq] + hi) * 256],
                v_all[lo * 256 : hi * 256, :],
                preferred_element_type=F32,
            )
            acc = part if acc is None else acc + part
        if not first:
            acc = acc + acc_in[rows, :] * jnp.concatenate([keep[zq], keep[zq]], axis=1)
        if last:
            whole[rows, :] = (acc[:, 0:128] / acc[:, 128:256]).astype(BF)
        else:
            acc_out[rows, :] = acc

    for step in STEPS:
        {"s": score, "w": weigh, "g": gather}[step[0]](int(step[1]))
    if last:
        for s in range(4):
            zs = lax.rem(at[0] + s, 4)
            chunks[s][...] = whole[pl.ds(pl.multiple_of(zs * 256, 256), 256), :]


def emit_body(at, *refs):
    att = refs[0:4]
    own_w, other_w = refs[4:8], refs[8:12]
    outs = refs[12:16]
    joined, weights, whole = refs[16:]
    z, y, c, x = at[0], at[1], at[2], at[3]
    for s in range(4):
        zs = slot_of(z, s, 4)
        joined[:, pl.ds(pl.multiple_of(zs * 128, 128), 128)] = att[s][...]
        for j in range(4):
            for k, w in ((c, own_w[j]), (1 - c, other_w[j])):
                ys = near(y, k, j)
                place = pl.ds(pl.multiple_of((zs * 8 + ys * 2 + k) * 32, 32), 32)
                weights[place, :] = w[s * 64 + 32 : s * 64 + 64, :]
    whole[...] = lax.dot_general(
        joined[...], weights[...], (((1,), (1,)), ((), ())), preferred_element_type=F32
    )
    for s in range(4):
        xs = lax.rem(x + s, 4)
        got = whole[pl.ds(pl.multiple_of(xs * 64, 64), 64), :]
        outs[s][...] = got.astype(outs[s].dtype)


def finish_body(at, own, r1, r2, r3, gain, out):
    total = own[...] + r1[...].astype(F32) + r2[...].astype(F32) + r3[...].astype(F32)
    mean = jnp.mean(total * total, axis=1, keepdims=True)
    out[...] = (total * lax.rsqrt(mean + 1e-06) * gain[...]).astype(BF)


def shape(*dims, dtype=BF):
    return jax.ShapeDtypeStruct(dims, dtype)


TURN = (2, 1, 3)


def ring(axis, values):
    got = [values[0], None, None, None]
    for s in TURN:
        got[s] = around(axis, s, values[s], 4)
    return got


CUM_AT = {
    (True, 0): (0, 0),
    (False, 0): (1, 0),
    (True, 1): (2, 0),
    (False, 2): (2, 32),
    (False, 1): (3, 0),
    (True, 2): (3, 32),
    (True, 3): (4, 0),
    (False, 3): (4, 32),
}
STEPS = ("s3", "s2", "w3", "g3", "s1", "w2", "g2", "s0", "w1", "g1", "w0", "g0")
GROUPS = (
    ((True, 0), (False, 0)),
    ((True, 2), (False, 2)),
    ((True, 1), (True, 3)),
    ((False, 1), (False, 3)),
)


def layer(tokens, wq, wk, wv, gate, forget_bias, out_weight, out_gain):
    bias = forget_bias.reshape(1, 4)
    seq_len = tokens.shape[0] * 128

    *first, a_own = named(pack_body, [shape(128, 512)] * 4 + [shape(64, 512)], first=True)(
        tokens, wq, wk, wv, gate.T, out_weight.T
    )
    a_x = spread("x", a_own)
    by_z = ring("z", first)

    mine = jnp.concatenate([m[64:128] for m in by_z], axis=0)
    own_w = spread("y", mine)
    b_half = spread("x", jnp.concatenate([m[0:64] for m in by_z], axis=0))
    a_half = spread("z", jnp.concatenate(a_x, axis=0))
    other_w = [around("c", 1, w, 2) for w in own_w]

    q, kv, cum = named(
        functools.partial(project_body, seq_len),
        [shape(1024, 128), shape(1024, 256), shape(32, 256)],
        [
            pltpu.VMEM((1024, 1024), BF),
            pltpu.VMEM((1024, 512), BF),
            pltpu.VMEM((8, 256), F32),
        ],
    )(bias, *a_half, *b_half, *own_w, *other_w)

    cum_mate = around("c", 1, cum, 2)
    cum_pair = jnp.concatenate([cum, cum_mate], axis=0)
    cum_near = along("y", 1, cum_pair)
    cum_far = around("y", 2, cum_pair, 4)
    cums = [cum, cum_mate, cum_near, around("c", 1, cum_near, 2), cum_far]
    kv_own = spread("y", kv, step=-1)
    where = {(True, j): kv_own[j] for j in range(4)}
    where |= {(False, j): around("c", 1, kv_own[j], 2) for j in range(4)}

    state = ()
    for g, slots in enumerate(GROUPS):
        n = len(slots)
        first_call, last_call = g == 0, g == len(GROUPS) - 1
        outs = (
            [shape(256, 128)] * 4
            if last_call
            else [shape(1024, 128, dtype=F32), shape(1024, 256, dtype=F32)]
        )
        state = named(
            functools.partial(attend_body, slots, first_call, last_call, 128 ** -0.5),
            outs,
            [
                pltpu.VMEM((n * 1024, 256), BF),
                pltpu.VMEM((256, n * 2560), F32),
                pltpu.VMEM((256, n * 2560), BF),
                pltpu.VMEM((1024, 128), BF),
            ],
        )(q, *cums, *[where[s] for s in slots], *state)

    att = ring("z", state)
    own, *rest = named(
        emit_body,
        [shape(64, 1024, dtype=F32)] + [shape(64, 1024)] * 3,
        [
            pltpu.VMEM((256, 512), BF),
            pltpu.VMEM((1024, 512), BF),
            pltpu.VMEM((256, 1024), F32),
        ],
    )(*att, *own_w, *other_w)
    got = ring("x", [own, *rest])
    (out,) = named(finish_body, [shape(64, 1024)], last=True)(
        *got, out_gain.reshape(1, 1024)
    )
    return out


def solution(mesh):
    torus = Mesh(mesh.devices.reshape(4, 4, 2, 4), ("z", "y", "c", "x"))
    sp = ("z", "y", "c")
    in_specs = (
        P(sp + ("x",), None),
        P(sp, "x"),
        P(sp, "x"),
        P(sp, "x"),
        P(sp, "x"),
        P("x"),
        P("x", sp),
        P(),
    )
    return jax.shard_map(
        layer, mesh=torus, in_specs=in_specs, out_specs=P(sp + ("x",), None), check_vma=False
    )
```

```python
import functools
import math

import jax
import jax.numpy as jnp
from jax import lax
from jax.experimental import pallas as pl
from jax.experimental.pallas import tpu as pltpu
from jax.sharding import Mesh
from jax.sharding import PartitionSpec as P


BF = jnp.bfloat16
F32 = jnp.float32
LOG2E = math.log2(math.e)
NEG = -1e30
VMEM = pl.BlockSpec(memory_space=pltpu.VMEM)


def named(body, outs, scratch=(), mib=20, first=False, last=False):
    space = pltpu.HBM if first else pltpu.VMEM

    def seated(*refs):
        body([lax.axis_index(axis) for axis in ("z", "y", "c", "x")], *refs)

    def run(*operands):
        return pl.pallas_call(
            seated,
            out_shape=outs if last else [pltpu.VMEM(o.shape, o.dtype) for o in outs],
            in_specs=[VMEM] * len(operands),
            out_specs=[VMEM] * len(outs),
            scratch_shapes=list(scratch),
            compiler_params=pltpu.CompilerParams(vmem_limit_bytes=mib * 1024 * 1024),
        )(*(pltpu.with_memory_space_constraint(o, space) for o in operands))

    return run


def around(axis, shift, value, size):
    return lax.ppermute(value, axis, [(i, (i + shift) % size) for i in range(size)])


def along(axis, step, value):
    names, index = ((axis, "c"), lambda i, c: 2 * (i % 4) + c)
    if axis == "x":
        names, index = (("c", "x"), lambda i, c: 4 * c + i % 4)
    pairs = [
        (index(i, c), index(i + (step, -step)[c], c)) for i in range(4) for c in range(2)
    ]
    return lax.ppermute(value, names, pairs)


def spread(axis, value, step=1):
    first = along(axis, step, value)
    second = along(axis, -step, value)
    pair = [first, second] if step == 1 else [second, first]
    return [value, *pair, along(axis, step, first)]


def near(index, core, slot):
    return lax.rem(index + (0, 3 + 2 * core, 1 + 2 * core, 2)[slot], 4)


def slot_of(index, shift, size):
    return lax.rem(index + (size - shift), size)


def pack_body(at, tok, wq, wk, wv, gate, ow, *outs):
    z = at[0]
    row4 = lax.broadcasted_iota(jnp.int32, (4, 32), 0)
    lane = lax.broadcasted_iota(jnp.int32, (32, 128), 1)
    gates = gate[...].astype(F32)
    for s in range(4):
        head = lax.rem(z + s, 4)
        o = outs[s]
        o[0:64, :] = tok[:, 512:1024]
        take = pl.ds(pl.multiple_of(head * 128, 128), 128)
        o[64:96, 0:128] = wq[:, take]
        o[64:96, 128:256] = wk[:, take]
        o[64:96, 256:384] = wv[:, take]
        line = jnp.sum(jnp.where(row4 == head, gates, 0.0), axis=0, keepdims=True)
        column = jnp.broadcast_to(line, (128, 32)).T
        o[64:96, 384:512] = jnp.where(lane == 0, column, 0.0).astype(BF)
        o[96:128, :] = ow[...]
    outs[4][...] = tok[:, 0:512]


def project_body(seq_len, at, *refs):
    bias, refs = refs[0], refs[1:]
    a_half, b_half = refs[0:4], refs[4:8]
    own_w, other_w = refs[8:12], refs[12:16]
    q_out, kv_out, cum_out = refs[16:19]
    toks, weights, gates = refs[19:]
    z, y, c, x = at[0], at[1], at[2], at[3]
    for s in range(4):
        zs = slot_of(z, s, 4)
        zn = near(z, c, s)
        for i in range(4):
            xs = near(x, c, i)
            place = pl.ds(pl.multiple_of((zn * 4 + xs) * 64, 64), 64)
            toks[place, 0:512] = a_half[s][i * 64 : (i + 1) * 64, :]
            place = pl.ds(pl.multiple_of((zs * 4 + xs) * 64, 64), 64)
            toks[place, 512:1024] = b_half[i][s * 64 : (s + 1) * 64, :]
        for j in range(4):
            for k, w in ((c, own_w[j]), (1 - c, other_w[j])):
                ys = near(y, k, j)
                place = pl.ds(pl.multiple_of((zs * 8 + ys * 2 + k) * 32, 32), 32)
                weights[place, :] = w[s * 64 : s * 64 + 32, :]
    whole = weights[...]
    for r in range(4):
        part = slice(r * 256, (r + 1) * 256)
        got = jnp.dot(toks[part, :], whole, preferred_element_type=F32)
        q_out[part, :] = got[:, 0:128].astype(BF)
        kv_out[part, :] = got[:, 128:384].astype(BF)
        gates[r : r + 1, :] = got[:, 384:512].T[0:1, :]
    gates[4:8, :] = jnp.zeros((4, 256), F32)
    spots = lax.broadcasted_iota(jnp.int32, (1, 4), 1)
    held = jnp.sum(jnp.where(spots == z, bias[...], 0.0), axis=1, keepdims=True)
    v = gates[...] + held + math.log(seq_len)
    u = jnp.exp(-jnp.abs(v))
    w1 = 1.0 + u
    soft = jnp.where(w1 == 1.0, u, jnp.log(w1) * (u / jnp.where(w1 == 1.0, 1.0, w1 - 1.0)))
    logs = jnp.minimum(v, 0.0) - soft
    upper = (
        lax.broadcasted_iota(jnp.int32, (256, 256), 0)
        <= lax.broadcasted_iota(jnp.int32, (256, 256), 1)
    ).astype(BF)
    total = jnp.zeros((8, 256), F32)
    for piece in in_parts(logs):
        total = total + jnp.dot(piece, upper, preferred_element_type=F32)
    pieces = in_parts(total)
    cum_out[0:16, :] = jnp.concatenate([pieces[0].astype(F32), pieces[1].astype(F32)]).astype(BF)
    cum_out[16:32, :] = jnp.concatenate(
        [pieces[2].astype(F32), jnp.zeros((8, 256), F32)]
    ).astype(BF)


def in_parts(value):
    high = value.astype(BF)
    rest = value - high.astype(F32)
    middle = rest.astype(BF)
    low = (rest - middle.astype(F32)).astype(BF)
    return high, middle, low


def attend_body(slots, first, last, scale, at, q, *refs):
    n = len(slots)
    cums, refs = refs[:5], refs[5:]
    kvs, refs = refs[:n], refs[n:]
    if first:
        m_in = acc_in = None
    else:
        m_in, acc_in = refs[:2]
        refs = refs[2:]
    if last:
        chunks = refs[:4]
        refs = refs[4:]
    else:
        m_out, acc_out = refs[:2]
        refs = refs[2:]
    v_all, scores, probs, whole = refs
    y, c = at[1], at[2]
    place = {}
    local = {}
    for s, (ref, start) in CUM_AT.items():
        got = cums[ref][start : start + 32, :].astype(F32)
        local[s] = got[0:8] + got[8:16] + got[16:24]
        core = c if s[0] else 1 - c
        place[s] = near(y, core, s[1]) * 2 + core
    ends = {s: local[s][:, 255:256] for s in local}
    row = lax.broadcasted_iota(jnp.int32, (8, 1), 0)
    every = functools.reduce(jnp.add, ends.values())
    before = jnp.zeros((8, 1), F32)
    for i in range(3):
        before = before + jnp.where(row > i, every[i : i + 1, :], 0.0)

    def absolute(s):
        inner = before
        for t in ends:
            inner = inner + jnp.where(place[t] < place[s], ends[t], 0.0)
        return (local[s] + inner) * LOG2E

    here = place[True, 0]
    own_cum = absolute((True, 0))
    bias_full, bias_edge = [], []
    for s in slots:
        b = own_cum if s == (True, 0) else absolute(s)
        bias_full.append(b)
        bias_edge.append(b if s == (True, 0) else jnp.where(place[s] < here, b, -NEG))
    ones = jnp.ones((256, 128), BF)
    for zk in range(4):
        for i in range(n):
            block = slice((zk * n + i) * 256, (zk * n + i + 1) * 256)
            v_all[block, 0:128] = kvs[i][zk * 256 : (zk + 1) * 256, 128:256]
            v_all[block, 128:256] = ones
    causal = lax.broadcasted_iota(jnp.int32, (256, 256), 1) <= lax.broadcasted_iota(
        jnp.int32, (256, 256), 0
    )
    begin = {3: 0, 2: 4 * n, 1: 7 * n, 0: 9 * n}
    shifts, keep = {}, {}

    def score(zq):
        rows = slice(zq * 256, (zq + 1) * 256)
        queries = q[rows, :]
        cum_t = jnp.broadcast_to(own_cum[zq : zq + 1, :], (128, 256)).T
        top = jnp.full((256, 128), NEG, F32)
        for zk in range(zq + 1):
            for i in range(n):
                b = begin[zq] + zk * n + i
                bias = (bias_edge if zk == zq else bias_full)[i][zk : zk + 1, :]
                got = (
                    lax.dot_general(
                        queries,
                        kvs[i][zk * 256 : (zk + 1) * 256, 0:128],
                        (((1,), (1,)), ((), ())),
                        preferred_element_type=F32,
                    )
                    * (scale * LOG2E)
                    - bias
                )
                if zk == zq and slots[i] == (True, 0):
                    got = jnp.where(causal, got, NEG)
                scores[:, b * 256 : (b + 1) * 256] = got
                top = jnp.maximum(top, jnp.maximum(got[:, 0:128], got[:, 128:256]))
        peak = jnp.broadcast_to(jnp.max(top, axis=1, keepdims=True), (256, 128)) + cum_t
        if not first:
            old = m_in[rows, :]
            peak = jnp.maximum(peak, old)
            keep[zq] = jnp.exp2(old - peak)
        shifts[zq] = cum_t - peak
        if not last:
            m_out[rows, :] = peak

    def weigh(zq):
        shift = jnp.concatenate([shifts[zq], shifts[zq]], axis=1)
        for b in range(begin[zq], begin[zq] + (zq + 1) * n):
            block = slice(b * 256, (b + 1) * 256)
            probs[:, block] = jnp.exp2(scores[:, block] + shift).astype(BF)

    def gather(zq):
        rows = slice(zq * 256, (zq + 1) * 256)
        blocks = (zq + 1) * n
        half = (blocks + 1) // 2
        acc = None
        for lo, hi in ((0, half), (half, blocks)):
            if lo == hi:
                continue
            part = jnp.dot(
                probs[:, (begin[zq] + lo) * 256 : (begin[zq] + hi) * 256],
                v_all[lo * 256 : hi * 256, :],
                preferred_element_type=F32,
            )
            acc = part if acc is None else acc + part
        if not first:
            acc = acc + acc_in[rows, :] * jnp.concatenate([keep[zq], keep[zq]], axis=1)
        if last:
            whole[rows, :] = (acc[:, 0:128] / acc[:, 128:256]).astype(BF)
        else:
            acc_out[rows, :] = acc

    for step in STEPS:
        {"s": score, "w": weigh, "g": gather}[step[0]](int(step[1]))
    if last:
        for s in range(4):
            zs = lax.rem(at[0] + s, 4)
            chunks[s][...] = whole[pl.ds(pl.multiple_of(zs * 256, 256), 256), :]


def emit_body(at, *refs):
    att = refs[0:4]
    own_w, other_w = refs[4:8], refs[8:12]
    outs = refs[12:16]
    joined, weights, whole = refs[16:]
    z, y, c, x = at[0], at[1], at[2], at[3]
    for s in range(4):
        zs = slot_of(z, s, 4)
        joined[:, pl.ds(pl.multiple_of(zs * 128, 128), 128)] = att[s][...]
        for j in range(4):
            for k, w in ((c, own_w[j]), (1 - c, other_w[j])):
                ys = near(y, k, j)
                place = pl.ds(pl.multiple_of((zs * 8 + ys * 2 + k) * 32, 32), 32)
                weights[place, :] = w[s * 64 + 32 : s * 64 + 64, :]
    whole[...] = lax.dot_general(
        joined[...], weights[...], (((1,), (1,)), ((), ())), preferred_element_type=F32
    )
    for s in range(4):
        xs = lax.rem(x + s, 4)
        got = whole[pl.ds(pl.multiple_of(xs * 64, 64), 64), :]
        outs[s][...] = got.astype(outs[s].dtype)


def finish_body(at, own, r1, r2, r3, gain, out):
    total = own[...] + r1[...].astype(F32) + r2[...].astype(F32) + r3[...].astype(F32)
    mean = jnp.mean(total * total, axis=1, keepdims=True)
    out[...] = (total * lax.rsqrt(mean + 1e-06) * gain[...]).astype(BF)


def shape(*dims, dtype=BF):
    return jax.ShapeDtypeStruct(dims, dtype)


TURN = (2, 1, 3)


def ring(axis, values):
    got = [values[0], None, None, None]
    for s in TURN:
        got[s] = around(axis, s, values[s], 4)
    return got


CUM_AT = {
    (True, 0): (0, 0),
    (False, 0): (1, 0),
    (True, 1): (2, 0),
    (False, 2): (2, 32),
    (False, 1): (3, 0),
    (True, 2): (3, 32),
    (True, 3): (4, 0),
    (False, 3): (4, 32),
}
STEPS = ("s3", "s2", "w3", "g3", "s1", "w2", "g2", "s0", "w1", "g1", "w0", "g0")
GROUPS = (
    ((True, 0), (False, 0)),
    ((True, 2), (False, 2)),
    ((True, 1),),
    ((False, 1), (True, 3)),
    ((False, 3),),
)


def layer(tokens, wq, wk, wv, gate, forget_bias, out_weight, out_gain):
    bias = forget_bias.reshape(1, 4)
    seq_len = tokens.shape[0] * 128

    *first, a_own = named(pack_body, [shape(128, 512)] * 4 + [shape(64, 512)], first=True)(
        tokens, wq, wk, wv, gate.T, out_weight.T
    )
    a_x = spread("x", a_own)
    by_z = ring("z", first)

    mine = jnp.concatenate([m[64:128] for m in by_z], axis=0)
    own_w = spread("y", mine)
    b_half = spread("x", jnp.concatenate([m[0:64] for m in by_z], axis=0))
    a_half = spread("z", jnp.concatenate(a_x, axis=0))
    other_w = [around("c", 1, w, 2) for w in own_w]

    q, kv, cum = named(
        functools.partial(project_body, seq_len),
        [shape(1024, 128), shape(1024, 256), shape(32, 256)],
        [
            pltpu.VMEM((1024, 1024), BF),
            pltpu.VMEM((1024, 512), BF),
            pltpu.VMEM((8, 256), F32),
        ],
    )(bias, *a_half, *b_half, *own_w, *other_w)

    cum_mate = around("c", 1, cum, 2)
    cum_pair = jnp.concatenate([cum, cum_mate], axis=0)
    cum_near = along("y", 1, cum_pair)
    cum_far = around("y", 2, cum_pair, 4)
    cums = [cum, cum_mate, cum_near, around("c", 1, cum_near, 2), cum_far]
    kv_own = spread("y", kv, step=-1)
    where = {(True, j): kv_own[j] for j in range(4)}
    where |= {(False, j): around("c", 1, kv_own[j], 2) for j in range(4)}

    state = ()
    for g, slots in enumerate(GROUPS):
        n = len(slots)
        first_call, last_call = g == 0, g == len(GROUPS) - 1
        outs = (
            [shape(256, 128)] * 4
            if last_call
            else [shape(1024, 128, dtype=F32), shape(1024, 256, dtype=F32)]
        )
        state = named(
            functools.partial(attend_body, slots, first_call, last_call, 128 ** -0.5),
            outs,
            [
                pltpu.VMEM((n * 1024, 256), BF),
                pltpu.VMEM((256, n * 2560), F32),
                pltpu.VMEM((256, n * 2560), BF),
                pltpu.VMEM((1024, 128), BF),
            ],
        )(q, *cums, *[where[s] for s in slots], *state)

    att = ring("z", state)
    own, *rest = named(
        emit_body,
        [shape(64, 1024, dtype=F32)] + [shape(64, 1024)] * 3,
        [
            pltpu.VMEM((256, 512), BF),
            pltpu.VMEM((1024, 512), BF),
            pltpu.VMEM((256, 1024), F32),
        ],
    )(*att, *own_w, *other_w)
    got = ring("x", [own, *rest])
    (out,) = named(finish_body, [shape(64, 1024)], last=True)(
        *got, out_gain.reshape(1, 1024)
    )
    return out


def solution(mesh):
    torus = Mesh(mesh.devices.reshape(4, 4, 2, 4), ("z", "y", "c", "x"))
    sp = ("z", "y", "c")
    in_specs = (
        P(sp + ("x",), None),
        P(sp, "x"),
        P(sp, "x"),
        P(sp, "x"),
        P(sp, "x"),
        P("x"),
        P("x", sp),
        P(),
    )
    return jax.shard_map(
        layer, mesh=torus, in_specs=in_specs, out_specs=P(sp + ("x",), None), check_vma=False
    )
```

```python
import functools
import math

import jax
import jax.numpy as jnp
from jax import lax
from jax.experimental import pallas as pl
from jax.experimental.pallas import tpu as pltpu
from jax.sharding import Mesh
from jax.sharding import PartitionSpec as P


BF = jnp.bfloat16
F32 = jnp.float32
LOG2E = math.log2(math.e)
NEG = -1e30
VMEM = pl.BlockSpec(memory_space=pltpu.VMEM)


def named(body, outs, scratch=(), mib=20, first=False, last=False, alias=None):
    space = pltpu.HBM if first else pltpu.VMEM

    def seated(*refs):
        body([lax.axis_index(axis) for axis in ("z", "y", "c", "x")], *refs)

    def run(*operands):
        return pl.pallas_call(
            seated,
            out_shape=outs if last else [pltpu.VMEM(o.shape, o.dtype) for o in outs],
            in_specs=[VMEM] * len(operands),
            out_specs=[VMEM] * len(outs),
            scratch_shapes=list(scratch),
            input_output_aliases=alias or {},
            compiler_params=pltpu.CompilerParams(vmem_limit_bytes=mib * 1024 * 1024),
        )(*(pltpu.with_memory_space_constraint(o, space) for o in operands))

    return run


def around(axis, shift, value, size):
    return lax.ppermute(value, axis, [(i, (i + shift) % size) for i in range(size)])


def along(axis, step, value):
    names, index = ((axis, "c"), lambda i, c: 2 * (i % 4) + c)
    if axis == "x":
        names, index = (("c", "x"), lambda i, c: 4 * c + i % 4)
    pairs = [
        (index(i, c), index(i + (step, -step)[c], c)) for i in range(4) for c in range(2)
    ]
    return lax.ppermute(value, names, pairs)


def spread(axis, value, step=1):
    first = along(axis, step, value)
    second = along(axis, -step, value)
    pair = [first, second] if step == 1 else [second, first]
    return [value, *pair, along(axis, step, first)]


def near(index, core, slot):
    return lax.rem(index + (0, 3 + 2 * core, 1 + 2 * core, 2)[slot], 4)


def slot_of(index, shift, size):
    return lax.rem(index + (size - shift), size)


def pack_body(at, tok, wq, wk, wv, gate, ow, *outs):
    z = at[0]
    row4 = lax.broadcasted_iota(jnp.int32, (4, 32), 0)
    lane = lax.broadcasted_iota(jnp.int32, (32, 128), 1)
    gates = gate[...].astype(F32)
    for s in range(4):
        head = lax.rem(z + s, 4)
        o = outs[s]
        o[0:64, :] = tok[:, 512:1024]
        take = pl.ds(pl.multiple_of(head * 128, 128), 128)
        o[64:96, 256:384] = wq[:, take]
        o[64:96, 0:128] = wk[:, take]
        o[64:96, 128:256] = wv[:, take]
        line = jnp.sum(jnp.where(row4 == head, gates, 0.0), axis=0, keepdims=True)
        column = jnp.broadcast_to(line, (128, 32)).T
        o[64:96, 384:512] = jnp.where(lane == 0, column, 0.0).astype(BF)
        o[96:128, :] = ow[...]
    outs[4][...] = tok[:, 0:512]


def lay_rows(at, slots, a_half, b_half, toks):
    z, c, x = at[0], at[2], at[3]
    for s, i in slots:
        xs = near(x, c, i)
        if a_half[s] is not None:
            place = (near(z, c, s) * 4 + xs) * 64
            place = pl.ds(pl.multiple_of(place, 64), 64)
            toks[place, 0:512] = a_half[s][i * 64 : (i + 1) * 64, :]
        if b_half[i] is not None:
            place = pl.ds(pl.multiple_of((slot_of(z, s, 4) * 4 + xs) * 64, 64), 64)
            toks[place, 512:1024] = b_half[i][s * 64 : (s + 1) * 64, :]


def lay_weights(at, slots, own_w, other_w, start, weights):
    z, y, c = at[0], at[1], at[2]
    for s in range(4):
        zs = slot_of(z, s, 4)
        for j in slots:
            for k, w in ((c, own_w[j]), (1 - c, other_w[j])):
                place = (zs * 8 + near(y, k, j) * 2 + k) * 32
                place = pl.ds(pl.multiple_of(place, 32), 32)
                weights[place, :] = w[s * 64 + start : s * 64 + start + 32, :]


EARLY = (0, 1, 2)
ALL = tuple((s, i) for s in range(4) for i in range(4))


def stack_body(at, *refs):
    lay_rows(at, ALL, (*refs[0:3], None), (*refs[3:6], None), refs[12])
    lay_weights(at, EARLY, refs[6:9], refs[9:12], 0, refs[13])


def lay_body(at, *refs):
    lay_weights(at, range(4), refs[0:4], refs[4:8], 32, refs[8])


def project_body(at, *refs):
    a_last, b_last, own_last, other_last = refs[0:4]
    kv_out, toks, weights = refs[6:9]
    lay_rows(at, ALL, (None, None, None, a_last), (None, None, None, b_last), toks)
    lay_weights(at, (3,), (None, None, None, own_last), (None, None, None, other_last), 0, weights)
    whole = weights[:, 0:256]
    for r in range(4):
        part = slice(r * 256, (r + 1) * 256)
        kv_out[part, :] = jnp.dot(
            toks[part, :], whole, preferred_element_type=F32
        ).astype(BF)


def query_body(seq_len, at, bias, toks, weights, q_out, cum_out, gates):
    z = at[0]
    whole = weights[:, 256:512]
    for r in range(4):
        part = slice(r * 256, (r + 1) * 256)
        got = jnp.dot(toks[part, :], whole, preferred_element_type=F32)
        q_out[part, :] = got[:, 0:128].astype(BF)
        gates[r : r + 1, :] = got[:, 128:256].T[0:1, :]
    gates[4:8, :] = jnp.zeros((4, 256), F32)
    spots = lax.broadcasted_iota(jnp.int32, (1, 4), 1)
    held = jnp.sum(jnp.where(spots == z, bias[...], 0.0), axis=1, keepdims=True)
    v = gates[...] + held + math.log(seq_len)
    u = jnp.exp(-jnp.abs(v))
    w1 = 1.0 + u
    soft = jnp.where(w1 == 1.0, u, jnp.log(w1) * (u / jnp.where(w1 == 1.0, 1.0, w1 - 1.0)))
    logs = jnp.minimum(v, 0.0) - soft
    upper = (
        lax.broadcasted_iota(jnp.int32, (256, 256), 0)
        <= lax.broadcasted_iota(jnp.int32, (256, 256), 1)
    ).astype(BF)
    total = jnp.zeros((8, 256), F32)
    for piece in in_parts(logs):
        total = total + jnp.dot(piece, upper, preferred_element_type=F32)
    pieces = in_parts(total)
    cum_out[0:16, :] = jnp.concatenate([pieces[0].astype(F32), pieces[1].astype(F32)]).astype(BF)
    cum_out[16:32, :] = jnp.concatenate(
        [pieces[2].astype(F32), jnp.zeros((8, 256), F32)]
    ).astype(BF)


def in_parts(value):
    high = value.astype(BF)
    rest = value - high.astype(F32)
    middle = rest.astype(BF)
    low = (rest - middle.astype(F32)).astype(BF)
    return high, middle, low


def attend_body(slots, first, last, scale, at, q, *refs):
    n = len(slots)
    cums, refs = refs[:5], refs[5:]
    kvs, refs = refs[:n], refs[n:]
    if first:
        m_in = acc_in = None
    else:
        m_in, acc_in = refs[:2]
        refs = refs[2:]
    if last:
        chunks = refs[:4]
        refs = refs[4:]
    else:
        m_out, acc_out = refs[:2]
        refs = refs[2:]
    v_all, scores, probs, whole = refs
    y, c = at[1], at[2]
    place = {}
    local = {}
    for s, (ref, start) in CUM_AT.items():
        got = cums[ref][start : start + 32, :].astype(F32)
        local[s] = got[0:8] + got[8:16] + got[16:24]
        core = c if s[0] else 1 - c
        place[s] = near(y, core, s[1]) * 2 + core
    ends = {s: local[s][:, 255:256] for s in local}
    row = lax.broadcasted_iota(jnp.int32, (8, 1), 0)
    every = functools.reduce(jnp.add, ends.values())
    before = jnp.zeros((8, 1), F32)
    for i in range(3):
        before = before + jnp.where(row > i, every[i : i + 1, :], 0.0)

    def absolute(s):
        inner = before
        for t in ends:
            inner = inner + jnp.where(place[t] < place[s], ends[t], 0.0)
        return (local[s] + inner) * LOG2E

    here = place[True, 0]
    own_cum = absolute((True, 0))
    bias_full, bias_edge = [], []
    for s in slots:
        b = own_cum if s == (True, 0) else absolute(s)
        bias_full.append(b)
        bias_edge.append(b if s == (True, 0) else jnp.where(place[s] < here, b, -NEG))
    ones = jnp.ones((256, 128), BF)
    for zk in range(4):
        for i in range(n):
            block = slice((zk * n + i) * 256, (zk * n + i + 1) * 256)
            v_all[block, 0:128] = kvs[i][zk * 256 : (zk + 1) * 256, 128:256]
            v_all[block, 128:256] = ones
    causal = lax.broadcasted_iota(jnp.int32, (256, 256), 1) <= lax.broadcasted_iota(
        jnp.int32, (256, 256), 0
    )
    begin = {3: 0, 2: 4 * n, 1: 7 * n, 0: 9 * n}
    shifts, keep = {}, {}

    def score(zq):
        rows = slice(zq * 256, (zq + 1) * 256)
        queries = q[rows, :]
        cum_t = jnp.broadcast_to(own_cum[zq : zq + 1, :], (128, 256)).T
        top = jnp.full((256, 128), NEG, F32)
        for zk in range(zq + 1):
            for i in range(n):
                b = begin[zq] + zk * n + i
                bias = (bias_edge if zk == zq else bias_full)[i][zk : zk + 1, :]
                got = (
                    lax.dot_general(
                        queries,
                        kvs[i][zk * 256 : (zk + 1) * 256, 0:128],
                        (((1,), (1,)), ((), ())),
                        preferred_element_type=F32,
                    )
                    * (scale * LOG2E)
                    - bias
                )
                if zk == zq and slots[i] == (True, 0):
                    got = jnp.where(causal, got, NEG)
                scores[:, b * 256 : (b + 1) * 256] = got
                top = jnp.maximum(top, jnp.maximum(got[:, 0:128], got[:, 128:256]))
        peak = jnp.broadcast_to(jnp.max(top, axis=1, keepdims=True), (256, 128)) + cum_t
        if not first:
            old = m_in[rows, :]
            peak = jnp.maximum(peak, old)
            keep[zq] = jnp.exp2(old - peak)
        shifts[zq] = cum_t - peak
        if not last:
            m_out[rows, :] = peak

    def weigh(zq):
        shift = jnp.concatenate([shifts[zq], shifts[zq]], axis=1)
        for b in range(begin[zq], begin[zq] + (zq + 1) * n):
            block = slice(b * 256, (b + 1) * 256)
            probs[:, block] = jnp.exp2(scores[:, block] + shift).astype(BF)

    def gather(zq):
        rows = slice(zq * 256, (zq + 1) * 256)
        blocks = (zq + 1) * n
        half = (blocks + 1) // 2
        acc = None
        for lo, hi in ((0, half), (half, blocks)):
            if lo == hi:
                continue
            part = jnp.dot(
                probs[:, (begin[zq] + lo) * 256 : (begin[zq] + hi) * 256],
                v_all[lo * 256 : hi * 256, :],
                preferred_element_type=F32,
            )
            acc = part if acc is None else acc + part
        if not first:
            acc = acc + acc_in[rows, :] * jnp.concatenate([keep[zq], keep[zq]], axis=1)
        if last:
            whole[rows, :] = (acc[:, 0:128] / acc[:, 128:256]).astype(BF)
        else:
            acc_out[rows, :] = acc

    for step in STEPS:
        {"s": score, "w": weigh, "g": gather}[step[0]](int(step[1]))
    if last:
        for s in range(4):
            zs = lax.rem(at[0] + s, 4)
            chunks[s][...] = whole[pl.ds(pl.multiple_of(zs * 256, 256), 256), :]


def emit_body(at, *refs):
    att, weights = refs[0:4], refs[4]
    outs = refs[5:9]
    joined, whole = refs[9:]
    z, x = at[0], at[3]
    for s in range(4):
        zs = slot_of(z, s, 4)
        joined[:, pl.ds(pl.multiple_of(zs * 128, 128), 128)] = att[s][...]
    whole[...] = lax.dot_general(
        joined[...], weights[...], (((1,), (1,)), ((), ())), preferred_element_type=F32
    )
    for s in range(4):
        xs = lax.rem(x + s, 4)
        got = whole[pl.ds(pl.multiple_of(xs * 64, 64), 64), :]
        outs[s][...] = got.astype(outs[s].dtype)


def finish_body(at, own, r1, r2, r3, gain, out):
    total = own[...] + r1[...].astype(F32) + r2[...].astype(F32) + r3[...].astype(F32)
    mean = jnp.mean(total * total, axis=1, keepdims=True)
    out[...] = (total * lax.rsqrt(mean + 1e-06) * gain[...]).astype(BF)


def shape(*dims, dtype=BF):
    return jax.ShapeDtypeStruct(dims, dtype)


TURN = (2, 1, 3)


def ring(axis, values):
    got = [values[0], None, None, None]
    for s in TURN:
        got[s] = around(axis, s, values[s], 4)
    return got


CUM_AT = {
    (True, 0): (0, 0),
    (False, 0): (1, 0),
    (True, 1): (2, 0),
    (False, 2): (2, 32),
    (False, 1): (3, 0),
    (True, 2): (3, 32),
    (True, 3): (4, 0),
    (False, 3): (4, 32),
}
STEPS = ("s3", "s2", "w3", "g3", "s1", "w2", "g2", "s0", "w1", "g1", "w0", "g0")
GROUPS = (
    ((True, 0), (False, 0)),
    ((True, 2), (False, 2)),
    ((True, 1),),
    ((False, 1), (True, 3)),
    ((False, 3),),
)


def layer(tokens, wq, wk, wv, gate, forget_bias, out_weight, out_gain):
    seq_len = tokens.shape[0] * 128

    *first, a_own = named(pack_body, [shape(128, 512)] * 4 + [shape(64, 512)], first=True)(
        tokens, wq, wk, wv, gate.T, out_weight.T
    )
    a_x = spread("x", a_own)
    by_z = ring("z", first)

    mine = jnp.concatenate([m[64:128] for m in by_z], axis=0)
    own_w = spread("y", mine)
    b_half = spread("x", jnp.concatenate([m[0:64] for m in by_z], axis=0))
    a_half = spread("z", jnp.concatenate(a_x, axis=0))
    other_w = [around("c", 1, w, 2) for w in own_w]

    early = named(stack_body, [shape(1024, 1024), shape(1024, 512)])(
        *a_half[:3], *b_half[:3], *own_w[:3], *other_w[:3]
    )
    kv, toks, weights = named(
        project_body,
        [shape(1024, 256), shape(1024, 1024), shape(1024, 512)],
        alias={4: 1, 5: 2},
    )(a_half[3], b_half[3], own_w[3], other_w[3], *early)
    q, cum = named(
        functools.partial(query_body, seq_len),
        [shape(1024, 128), shape(32, 256)],
        [pltpu.VMEM((8, 256), F32)],
    )(forget_bias.reshape(1, 4), toks, weights)

    cum_mate = around("c", 1, cum, 2)
    cum_pair = jnp.concatenate([cum, cum_mate], axis=0)
    cum_near = along("y", 1, cum_pair)
    cum_far = around("y", 2, cum_pair, 4)
    cums = [cum, cum_mate, cum_near, around("c", 1, cum_near, 2), cum_far]
    kv_own = spread("y", kv, step=-1)
    where = {(True, j): kv_own[j] for j in range(4)}
    where |= {(False, j): around("c", 1, kv_own[j], 2) for j in range(4)}

    state = ()
    for g, slots in enumerate(GROUPS):
        n = len(slots)
        first_call, last_call = g == 0, g == len(GROUPS) - 1
        outs = (
            [shape(256, 128)] * 4
            if last_call
            else [shape(1024, 128, dtype=F32), shape(1024, 256, dtype=F32)]
        )
        state = named(
            functools.partial(attend_body, slots, first_call, last_call, 128 ** -0.5),
            outs,
            [
                pltpu.VMEM((n * 1024, 256), BF),
                pltpu.VMEM((256, n * 2560), F32),
                pltpu.VMEM((256, n * 2560), BF),
                pltpu.VMEM((1024, 128), BF),
            ],
        )(q, *cums, *[where[s] for s in slots], *state)

    att = ring("z", state)
    laid = named(lay_body, [shape(1024, 512)])(*own_w, *other_w)
    own, *rest = named(
        emit_body,
        [shape(64, 1024, dtype=F32)] + [shape(64, 1024)] * 3,
        [
            pltpu.VMEM((256, 512), BF),
            pltpu.VMEM((256, 1024), F32),
        ],
    )(*att, *laid)
    got = ring("x", [own, *rest])
    (out,) = named(finish_body, [shape(64, 1024)], last=True)(
        *got, out_gain.reshape(1, 1024)
    )
    return out


def solution(mesh):
    torus = Mesh(mesh.devices.reshape(4, 4, 2, 4), ("z", "y", "c", "x"))
    sp = ("z", "y", "c")
    in_specs = (
        P(sp + ("x",), None),
        P(sp, "x"),
        P(sp, "x"),
        P(sp, "x"),
        P(sp, "x"),
        P("x"),
        P("x", sp),
        P(),
    )
    return jax.shard_map(
        layer, mesh=torus, in_specs=in_specs, out_specs=P(sp + ("x",), None), check_vma=False
    )
```

```python
import functools
import math

import jax
import jax.numpy as jnp
from jax import lax
from jax.experimental import pallas as pl
from jax.experimental.pallas import tpu as pltpu
from jax.sharding import Mesh
from jax.sharding import PartitionSpec as P


BF = jnp.bfloat16
F32 = jnp.float32
LOG2E = math.log2(math.e)
NEG = -1e30
VMEM = pl.BlockSpec(memory_space=pltpu.VMEM)


def named(body, outs, scratch=(), mib=20, first=False, last=False, alias=None):
    space = pltpu.HBM if first else pltpu.VMEM

    def seated(*refs):
        body([lax.axis_index(axis) for axis in ("z", "y", "c", "x")], *refs)

    def run(*operands):
        return pl.pallas_call(
            seated,
            out_shape=outs if last else [pltpu.VMEM(o.shape, o.dtype) for o in outs],
            in_specs=[VMEM] * len(operands),
            out_specs=[VMEM] * len(outs),
            scratch_shapes=list(scratch),
            input_output_aliases=alias or {},
            compiler_params=pltpu.CompilerParams(vmem_limit_bytes=mib * 1024 * 1024),
        )(*(pltpu.with_memory_space_constraint(o, space) for o in operands))

    return run


def around(axis, shift, value, size):
    return lax.ppermute(value, axis, [(i, (i + shift) % size) for i in range(size)])


def along(axis, step, value):
    names, index = ((axis, "c"), lambda i, c: 2 * (i % 4) + c)
    if axis == "x":
        names, index = (("c", "x"), lambda i, c: 4 * c + i % 4)
    pairs = [
        (index(i, c), index(i + (step, -step)[c], c)) for i in range(4) for c in range(2)
    ]
    return lax.ppermute(value, names, pairs)


def spread(axis, value, step=1):
    first = along(axis, step, value)
    second = along(axis, -step, value)
    pair = [first, second] if step == 1 else [second, first]
    return [value, *pair, along(axis, step, first)]


def near(index, core, slot):
    return lax.rem(index + (0, 3 + 2 * core, 1 + 2 * core, 2)[slot], 4)


def slot_of(index, shift, size):
    return lax.rem(index + (size - shift), size)


def pack_body(at, tok, wq, wk, wv, gate, ow, *outs):
    z = at[0]
    row4 = lax.broadcasted_iota(jnp.int32, (4, 32), 0)
    lane = lax.broadcasted_iota(jnp.int32, (32, 128), 1)
    gates = gate[...].astype(F32)
    for s in range(4):
        head = lax.rem(z + s, 4)
        o = outs[s]
        o[0:64, :] = tok[:, 512:1024]
        take = pl.ds(pl.multiple_of(head * 128, 128), 128)
        o[64:96, 256:384] = wq[:, take]
        o[64:96, 0:128] = wk[:, take]
        o[64:96, 128:256] = wv[:, take]
        line = jnp.sum(jnp.where(row4 == head, gates, 0.0), axis=0, keepdims=True)
        column = jnp.broadcast_to(line, (128, 32)).T
        o[64:96, 384:512] = jnp.where(lane == 0, column, 0.0).astype(BF)
        o[96:128, :] = ow[...]
    outs[4][...] = tok[:, 0:512]


def lay_rows(at, slots, a_half, b_half, toks):
    z, c, x = at[0], at[2], at[3]
    for s, i in slots:
        xs = near(x, c, i)
        if a_half[s] is not None:
            place = (near(z, c, s) * 4 + xs) * 64
            place = pl.ds(pl.multiple_of(place, 64), 64)
            toks[place, 0:512] = a_half[s][i * 64 : (i + 1) * 64, :]
        if b_half[i] is not None:
            place = pl.ds(pl.multiple_of((slot_of(z, s, 4) * 4 + xs) * 64, 64), 64)
            toks[place, 512:1024] = b_half[i][s * 64 : (s + 1) * 64, :]


def lay_weights(at, slots, own_w, other_w, start, weights):
    z, y, c = at[0], at[1], at[2]
    for s in range(4):
        zs = slot_of(z, s, 4)
        for j in slots:
            for k, w in ((c, own_w[j]), (1 - c, other_w[j])):
                place = (zs * 8 + near(y, k, j) * 2 + k) * 32
                place = pl.ds(pl.multiple_of(place, 32), 32)
                weights[place, :] = w[s * 64 + start : s * 64 + start + 32, :]


EARLY = (0, 1, 2)
ALL = tuple((s, i) for s in range(4) for i in range(4))


def stack_body(at, *refs):
    lay_rows(at, ALL, (*refs[0:3], None), (*refs[3:6], None), refs[12])
    lay_weights(at, EARLY, refs[6:9], refs[9:12], 0, refs[13])


def lay_body(at, *refs):
    lay_weights(at, range(4), refs[0:4], refs[4:8], 32, refs[8])


def project_body(at, *refs):
    a_last, b_last, own_last, other_last = refs[0:4]
    kv_out, toks, weights = refs[6:9]
    lay_rows(at, ALL, (None, None, None, a_last), (None, None, None, b_last), toks)
    lay_weights(at, (3,), (None, None, None, own_last), (None, None, None, other_last), 0, weights)
    whole = weights[:, 0:256]
    for r in range(4):
        part = slice(r * 256, (r + 1) * 256)
        kv_out[part, :] = jnp.dot(
            toks[part, :], whole, preferred_element_type=F32
        ).astype(BF)


def query_body(seq_len, at, bias, toks, weights, q_out, cum_out, gates):
    z = at[0]
    whole = weights[:, 256:512]
    for r in range(4):
        part = slice(r * 256, (r + 1) * 256)
        got = jnp.dot(toks[part, :], whole, preferred_element_type=F32)
        q_out[part, :] = got[:, 0:128].astype(BF)
        gates[r : r + 1, :] = got[:, 128:256].T[0:1, :]
    gates[4:8, :] = jnp.zeros((4, 256), F32)
    spots = lax.broadcasted_iota(jnp.int32, (1, 4), 1)
    held = jnp.sum(jnp.where(spots == z, bias[...], 0.0), axis=1, keepdims=True)
    v = gates[...] + held + math.log(seq_len)
    u = jnp.exp(-jnp.abs(v))
    w1 = 1.0 + u
    soft = jnp.where(w1 == 1.0, u, jnp.log(w1) * (u / jnp.where(w1 == 1.0, 1.0, w1 - 1.0)))
    logs = jnp.minimum(v, 0.0) - soft
    upper = (
        lax.broadcasted_iota(jnp.int32, (256, 256), 0)
        <= lax.broadcasted_iota(jnp.int32, (256, 256), 1)
    ).astype(BF)
    total = jnp.zeros((8, 256), F32)
    for piece in in_parts(logs):
        total = total + jnp.dot(piece, upper, preferred_element_type=F32)
    pieces = in_parts(total)
    cum_out[0:16, :] = jnp.concatenate([pieces[0].astype(F32), pieces[1].astype(F32)]).astype(BF)
    cum_out[16:32, :] = jnp.concatenate(
        [pieces[2].astype(F32), jnp.zeros((8, 256), F32)]
    ).astype(BF)


def in_parts(value):
    high = value.astype(BF)
    rest = value - high.astype(F32)
    middle = rest.astype(BF)
    low = (rest - middle.astype(F32)).astype(BF)
    return high, middle, low


def attend_body(slots, first, last, scale, at, q, *refs):
    n = len(slots)
    cums, refs = refs[:5], refs[5:]
    kvs, refs = refs[:n], refs[n:]
    if first:
        m_in = acc_in = None
    else:
        m_in, acc_in = refs[:2]
        refs = refs[2:]
    if last:
        chunks = refs[:4]
        refs = refs[4:]
    else:
        m_out, acc_out = refs[:2]
        refs = refs[2:]
    v_all, scores, probs, whole = refs
    y, c = at[1], at[2]
    place = {}
    local = {}
    for s, (ref, start) in CUM_AT.items():
        got = cums[ref][start : start + 32, :].astype(F32)
        local[s] = got[0:8] + got[8:16] + got[16:24]
        core = c if s[0] else 1 - c
        place[s] = near(y, core, s[1]) * 2 + core
    ends = {s: local[s][:, 255:256] for s in local}
    row = lax.broadcasted_iota(jnp.int32, (8, 1), 0)
    every = functools.reduce(jnp.add, ends.values())
    before = jnp.zeros((8, 1), F32)
    for i in range(3):
        before = before + jnp.where(row > i, every[i : i + 1, :], 0.0)

    def absolute(s):
        inner = before
        for t in ends:
            inner = inner + jnp.where(place[t] < place[s], ends[t], 0.0)
        return (local[s] + inner) * LOG2E

    here = place[True, 0]
    own_cum = absolute((True, 0))
    bias_full, bias_edge = [], []
    for s in slots:
        b = own_cum if s == (True, 0) else absolute(s)
        bias_full.append(b)
        bias_edge.append(b if s == (True, 0) else jnp.where(place[s] < here, b, -NEG))
    ones = jnp.ones((256, 128), BF)
    for zk in range(4):
        for i in range(n):
            block = slice((zk * n + i) * 256, (zk * n + i + 1) * 256)
            v_all[block, 0:128] = kvs[i][zk * 256 : (zk + 1) * 256, 128:256]
            v_all[block, 128:256] = ones
    causal = lax.broadcasted_iota(jnp.int32, (256, 256), 1) <= lax.broadcasted_iota(
        jnp.int32, (256, 256), 0
    )
    begin = {3: 0, 2: 4 * n, 1: 7 * n, 0: 9 * n}
    shifts, keep = {}, {}

    def score(zq):
        rows = slice(zq * 256, (zq + 1) * 256)
        queries = q[rows, :]
        cum_t = jnp.broadcast_to(own_cum[zq : zq + 1, :], (128, 256)).T
        tops = []
        for half in range(2):
            lines = slice(half * 128, (half + 1) * 128)
            top = jnp.full((128, 128), NEG, F32)
            for zk in range(zq + 1):
                for i in range(n):
                    b = begin[zq] + zk * n + i
                    bias = (bias_edge if zk == zq else bias_full)[i][zk : zk + 1, :]
                    got = (
                        lax.dot_general(
                            queries[lines],
                            kvs[i][zk * 256 : (zk + 1) * 256, 0:128],
                            (((1,), (1,)), ((), ())),
                            preferred_element_type=F32,
                        )
                        * (scale * LOG2E)
                        - bias
                    )
                    if zk == zq and slots[i] == (True, 0):
                        got = jnp.where(causal[lines], got, NEG)
                    scores[lines, b * 256 : (b + 1) * 256] = got
                    top = jnp.maximum(top, jnp.maximum(got[:, 0:128], got[:, 128:256]))
            tops.append(top)
        top = jnp.concatenate(tops, axis=0)
        peak = jnp.broadcast_to(jnp.max(top, axis=1, keepdims=True), (256, 128)) + cum_t
        if not first:
            old = m_in[rows, :]
            peak = jnp.maximum(peak, old)
            keep[zq] = jnp.exp2(old - peak)
        shifts[zq] = cum_t - peak
        if not last:
            m_out[rows, :] = peak

    def weigh(zq):
        shift = jnp.concatenate([shifts[zq], shifts[zq]], axis=1)
        for b in range(begin[zq], begin[zq] + (zq + 1) * n):
            block = slice(b * 256, (b + 1) * 256)
            probs[:, block] = jnp.exp2(scores[:, block] + shift).astype(BF)

    def gather(zq):
        rows = slice(zq * 256, (zq + 1) * 256)
        blocks = (zq + 1) * n
        half = (blocks + 1) // 2
        acc = None
        for lo, hi in ((0, half), (half, blocks)):
            if lo == hi:
                continue
            part = jnp.dot(
                probs[:, (begin[zq] + lo) * 256 : (begin[zq] + hi) * 256],
                v_all[lo * 256 : hi * 256, :],
                preferred_element_type=F32,
            )
            acc = part if acc is None else acc + part
        if not first:
            acc = acc + acc_in[rows, :] * jnp.concatenate([keep[zq], keep[zq]], axis=1)
        if last:
            whole[rows, :] = (acc[:, 0:128] / acc[:, 128:256]).astype(BF)
        else:
            acc_out[rows, :] = acc

    for step in STEPS:
        {"s": score, "w": weigh, "g": gather}[step[0]](int(step[1]))
    if last:
        for s in range(4):
            zs = lax.rem(at[0] + s, 4)
            chunks[s][...] = whole[pl.ds(pl.multiple_of(zs * 256, 256), 256), :]


def emit_body(at, *refs):
    att, weights = refs[0:4], refs[4]
    outs = refs[5:9]
    joined, whole = refs[9:]
    z, x = at[0], at[3]
    for s in range(4):
        zs = slot_of(z, s, 4)
        joined[:, pl.ds(pl.multiple_of(zs * 128, 128), 128)] = att[s][...]
    whole[...] = lax.dot_general(
        joined[...], weights[...], (((1,), (1,)), ((), ())), preferred_element_type=F32
    )
    for s in range(4):
        xs = lax.rem(x + s, 4)
        got = whole[pl.ds(pl.multiple_of(xs * 64, 64), 64), :]
        outs[s][...] = got.astype(outs[s].dtype)


def finish_body(at, own, r1, r2, r3, gain, out):
    total = own[...] + r1[...].astype(F32) + r2[...].astype(F32) + r3[...].astype(F32)
    mean = jnp.mean(total * total, axis=1, keepdims=True)
    out[...] = (total * lax.rsqrt(mean + 1e-06) * gain[...]).astype(BF)


def shape(*dims, dtype=BF):
    return jax.ShapeDtypeStruct(dims, dtype)


TURN = (2, 1, 3)


def ring(axis, values):
    got = [values[0], None, None, None]
    for s in TURN:
        got[s] = around(axis, s, values[s], 4)
    return got


CUM_AT = {
    (True, 0): (0, 0),
    (False, 0): (1, 0),
    (True, 1): (2, 0),
    (False, 2): (2, 32),
    (False, 1): (3, 0),
    (True, 2): (3, 32),
    (True, 3): (4, 0),
    (False, 3): (4, 32),
}
STEPS = ("s3", "s2", "w3", "g3", "s1", "w2", "g2", "s0", "w1", "g1", "w0", "g0")
GROUPS = (
    ((True, 0), (False, 0)),
    ((True, 2), (False, 2)),
    ((True, 1),),
    ((False, 1), (True, 3)),
    ((False, 3),),
)


def layer(tokens, wq, wk, wv, gate, forget_bias, out_weight, out_gain):
    seq_len = tokens.shape[0] * 128

    *first, a_own = named(pack_body, [shape(128, 512)] * 4 + [shape(64, 512)], first=True)(
        tokens, wq, wk, wv, gate.T, out_weight.T
    )
    a_x = spread("x", a_own)
    by_z = ring("z", first)

    mine = jnp.concatenate([m[64:128] for m in by_z], axis=0)
    own_w = spread("y", mine)
    b_half = spread("x", jnp.concatenate([m[0:64] for m in by_z], axis=0))
    a_half = spread("z", jnp.concatenate(a_x, axis=0))
    other_w = [around("c", 1, w, 2) for w in own_w]

    early = named(stack_body, [shape(1024, 1024), shape(1024, 512)])(
        *a_half[:3], *b_half[:3], *own_w[:3], *other_w[:3]
    )
    kv, toks, weights = named(
        project_body,
        [shape(1024, 256), shape(1024, 1024), shape(1024, 512)],
        alias={4: 1, 5: 2},
    )(a_half[3], b_half[3], own_w[3], other_w[3], *early)
    q, cum = named(
        functools.partial(query_body, seq_len),
        [shape(1024, 128), shape(32, 256)],
        [pltpu.VMEM((8, 256), F32)],
    )(forget_bias.reshape(1, 4), toks, weights)

    cum_mate = around("c", 1, cum, 2)
    cum_pair = jnp.concatenate([cum, cum_mate], axis=0)
    cum_near = along("y", 1, cum_pair)
    cum_far = around("y", 2, cum_pair, 4)
    cums = [cum, cum_mate, cum_near, around("c", 1, cum_near, 2), cum_far]
    kv_own = spread("y", kv, step=-1)
    where = {(True, j): kv_own[j] for j in range(4)}
    where |= {(False, j): around("c", 1, kv_own[j], 2) for j in range(4)}

    state = ()
    for g, slots in enumerate(GROUPS):
        n = len(slots)
        first_call, last_call = g == 0, g == len(GROUPS) - 1
        outs = (
            [shape(256, 128)] * 4
            if last_call
            else [shape(1024, 128, dtype=F32), shape(1024, 256, dtype=F32)]
        )
        state = named(
            functools.partial(attend_body, slots, first_call, last_call, 128 ** -0.5),
            outs,
            [
                pltpu.VMEM((n * 1024, 256), BF),
                pltpu.VMEM((256, n * 2560), F32),
                pltpu.VMEM((256, n * 2560), BF),
                pltpu.VMEM((1024, 128), BF),
            ],
        )(q, *cums, *[where[s] for s in slots], *state)

    att = ring("z", state)
    laid = named(lay_body, [shape(1024, 512)])(*own_w, *other_w)
    own, *rest = named(
        emit_body,
        [shape(64, 1024, dtype=F32)] + [shape(64, 1024)] * 3,
        [
            pltpu.VMEM((256, 512), BF),
            pltpu.VMEM((256, 1024), F32),
        ],
    )(*att, *laid)
    got = ring("x", [own, *rest])
    (out,) = named(finish_body, [shape(64, 1024)], last=True)(
        *got, out_gain.reshape(1, 1024)
    )
    return out


def solution(mesh):
    torus = Mesh(mesh.devices.reshape(4, 4, 2, 4), ("z", "y", "c", "x"))
    sp = ("z", "y", "c")
    in_specs = (
        P(sp + ("x",), None),
        P(sp, "x"),
        P(sp, "x"),
        P(sp, "x"),
        P(sp, "x"),
        P("x"),
        P("x", sp),
        P(),
    )
    return jax.shard_map(
        layer, mesh=torus, in_specs=in_specs, out_specs=P(sp + ("x",), None), check_vma=False
    )
```

```python
import functools
import math

import jax
import jax.numpy as jnp
from jax import lax
from jax.experimental import pallas as pl
from jax.experimental.pallas import tpu as pltpu
from jax.sharding import Mesh
from jax.sharding import PartitionSpec as P


BF = jnp.bfloat16
F32 = jnp.float32
LOG2E = math.log2(math.e)
NEG = -1e30
VMEM = pl.BlockSpec(memory_space=pltpu.VMEM)


def named(body, outs, scratch=(), mib=32, first=False, last=False, alias=None):
    space = pltpu.HBM if first else pltpu.VMEM

    def seated(*refs):
        body([lax.axis_index(axis) for axis in ("z", "y", "c", "x")], *refs)

    def run(*operands):
        return pl.pallas_call(
            seated,
            out_shape=outs if last else [pltpu.VMEM(o.shape, o.dtype) for o in outs],
            in_specs=[VMEM] * len(operands),
            out_specs=[VMEM] * len(outs),
            scratch_shapes=list(scratch),
            input_output_aliases=alias or {},
            compiler_params=pltpu.CompilerParams(vmem_limit_bytes=mib * 1024 * 1024),
        )(*(pltpu.with_memory_space_constraint(o, space) for o in operands))

    return run


def around(axis, shift, value, size):
    return lax.ppermute(value, axis, [(i, (i + shift) % size) for i in range(size)])


def along(axis, step, value):
    names, index = ((axis, "c"), lambda i, c: 2 * (i % 4) + c)
    if axis == "x":
        names, index = (("c", "x"), lambda i, c: 4 * c + i % 4)
    pairs = [
        (index(i, c), index(i + (step, -step)[c], c)) for i in range(4) for c in range(2)
    ]
    return lax.ppermute(value, names, pairs)


def spread(axis, value, step=1):
    first = along(axis, step, value)
    second = along(axis, -step, value)
    pair = [first, second] if step == 1 else [second, first]
    return [value, *pair, along(axis, step, first)]


def near(index, core, slot):
    return lax.rem(index + (0, 3 + 2 * core, 1 + 2 * core, 2)[slot], 4)


def slot_of(index, shift, size):
    return lax.rem(index + (size - shift), size)


def pack_body(at, tok, wq, wk, wv, gate, ow, *outs):
    z = at[0]
    row4 = lax.broadcasted_iota(jnp.int32, (4, 32), 0)
    lane = lax.broadcasted_iota(jnp.int32, (32, 128), 1)
    gates = gate[...].astype(F32)
    for s in range(4):
        head = lax.rem(z + s, 4)
        o = outs[s]
        o[0:64, :] = tok[:, 512:1024]
        take = pl.ds(pl.multiple_of(head * 128, 128), 128)
        o[64:96, 256:384] = wq[:, take]
        o[64:96, 0:128] = wk[:, take]
        o[64:96, 128:256] = wv[:, take]
        line = jnp.sum(jnp.where(row4 == head, gates, 0.0), axis=0, keepdims=True)
        column = jnp.broadcast_to(line, (128, 32)).T
        o[64:96, 384:512] = jnp.where(lane == 0, column, 0.0).astype(BF)
        o[96:128, :] = ow[...]
    outs[4][...] = tok[:, 0:512]


def lay_rows(at, slots, a_half, b_half, toks):
    z, c, x = at[0], at[2], at[3]
    for s, i in slots:
        xs = near(x, c, i)
        if a_half[s] is not None:
            place = (near(z, c, s) * 4 + xs) * 64
            place = pl.ds(pl.multiple_of(place, 64), 64)
            toks[place, 0:512] = a_half[s][i * 64 : (i + 1) * 64, :]
        if b_half[i] is not None:
            place = pl.ds(pl.multiple_of((slot_of(z, s, 4) * 4 + xs) * 64, 64), 64)
            toks[place, 512:1024] = b_half[i][s * 64 : (s + 1) * 64, :]


def lay_weights(at, slots, own_w, other_w, start, weights):
    z, y, c = at[0], at[1], at[2]
    for s in range(4):
        zs = slot_of(z, s, 4)
        for j in slots:
            for k, w in ((c, own_w[j]), (1 - c, other_w[j])):
                place = (zs * 8 + near(y, k, j) * 2 + k) * 32
                place = pl.ds(pl.multiple_of(place, 32), 32)
                weights[place, :] = w[s * 64 + start : s * 64 + start + 32, :]


EARLY = (0, 1, 2)
ALL = tuple((s, i) for s in range(4) for i in range(4))


def stack_body(at, *refs):
    lay_rows(at, ALL, (*refs[0:3], None), (*refs[3:6], None), refs[12])
    lay_weights(at, EARLY, refs[6:9], refs[9:12], 0, refs[13])


def lay_body(at, *refs):
    lay_weights(at, range(4), refs[0:4], refs[4:8], 32, refs[8])


def project_body(at, *refs):
    a_last, b_last, own_last, other_last = refs[0:4]
    kv_out, toks, weights = refs[6:9]
    lay_rows(at, ALL, (None, None, None, a_last), (None, None, None, b_last), toks)
    lay_weights(at, (3,), (None, None, None, own_last), (None, None, None, other_last), 0, weights)
    whole = weights[:, 0:256]
    for r in range(4):
        part = slice(r * 256, (r + 1) * 256)
        kv_out[part, :] = jnp.dot(
            toks[part, :], whole, preferred_element_type=F32
        ).astype(BF)


def query_body(seq_len, at, bias, toks, weights, q_out, cum_out, gates):
    z = at[0]
    whole = weights[:, 256:512]
    for r in range(4):
        part = slice(r * 256, (r + 1) * 256)
        got = jnp.dot(toks[part, :], whole, preferred_element_type=F32)
        q_out[part, :] = got[:, 0:128].astype(BF)
        gates[r : r + 1, :] = got[:, 128:256].T[0:1, :]
    gates[4:8, :] = jnp.zeros((4, 256), F32)
    spots = lax.broadcasted_iota(jnp.int32, (1, 4), 1)
    held = jnp.sum(jnp.where(spots == z, bias[...], 0.0), axis=1, keepdims=True)
    v = gates[...] + held + math.log(seq_len)
    u = jnp.exp(-jnp.abs(v))
    w1 = 1.0 + u
    soft = jnp.where(w1 == 1.0, u, jnp.log(w1) * (u / jnp.where(w1 == 1.0, 1.0, w1 - 1.0)))
    logs = jnp.minimum(v, 0.0) - soft
    upper = (
        lax.broadcasted_iota(jnp.int32, (256, 256), 0)
        <= lax.broadcasted_iota(jnp.int32, (256, 256), 1)
    ).astype(BF)
    total = jnp.zeros((8, 256), F32)
    for piece in in_parts(logs):
        total = total + jnp.dot(piece, upper, preferred_element_type=F32)
    pieces = in_parts(total)
    cum_out[0:16, :] = jnp.concatenate([pieces[0].astype(F32), pieces[1].astype(F32)]).astype(BF)
    cum_out[16:32, :] = jnp.concatenate(
        [pieces[2].astype(F32), jnp.zeros((8, 256), F32)]
    ).astype(BF)


def in_parts(value):
    high = value.astype(BF)
    rest = value - high.astype(F32)
    middle = rest.astype(BF)
    low = (rest - middle.astype(F32)).astype(BF)
    return high, middle, low


def attend_body(slots, first, last, scale, at, q, *refs):
    n = len(slots)
    cums, refs = refs[:5], refs[5:]
    kvs, refs = refs[:n], refs[n:]
    if first:
        m_in = acc_in = None
    else:
        m_in, acc_in = refs[:2]
        refs = refs[2:]
    if last:
        chunks = refs[:4]
        refs = refs[4:]
    else:
        m_out, acc_out = refs[:2]
        refs = refs[2:]
    v_all, scores, probs, whole = refs
    y, c = at[1], at[2]
    place = {}
    local = {}
    for s, (ref, start) in CUM_AT.items():
        got = cums[ref][start : start + 32, :].astype(F32)
        local[s] = got[0:8] + got[8:16] + got[16:24]
        core = c if s[0] else 1 - c
        place[s] = near(y, core, s[1]) * 2 + core
    ends = {s: local[s][:, 255:256] for s in local}
    row = lax.broadcasted_iota(jnp.int32, (8, 1), 0)
    every = functools.reduce(jnp.add, ends.values())
    before = jnp.zeros((8, 1), F32)
    for i in range(3):
        before = before + jnp.where(row > i, every[i : i + 1, :], 0.0)

    def absolute(s):
        inner = before
        for t in ends:
            inner = inner + jnp.where(place[t] < place[s], ends[t], 0.0)
        return (local[s] + inner) * LOG2E

    here = place[True, 0]
    own_cum = absolute((True, 0))
    bias_full, bias_edge = [], []
    for s in slots:
        b = own_cum if s == (True, 0) else absolute(s)
        bias_full.append(b)
        bias_edge.append(b if s == (True, 0) else jnp.where(place[s] < here, b, -NEG))
    ones = jnp.ones((256, 128), BF)
    for zk in range(4):
        for i in range(n):
            block = slice((zk * n + i) * 256, (zk * n + i + 1) * 256)
            v_all[block, 0:128] = kvs[i][zk * 256 : (zk + 1) * 256, 128:256]
            v_all[block, 128:256] = ones
    causal = lax.broadcasted_iota(jnp.int32, (256, 256), 1) <= lax.broadcasted_iota(
        jnp.int32, (256, 256), 0
    )
    begin = {3: 0, 2: 4 * n, 1: 7 * n, 0: 9 * n}
    shifts, keep = {}, {}

    def score(zq):
        rows = slice(zq * 256, (zq + 1) * 256)
        queries = q[rows, :]
        cum_t = jnp.broadcast_to(own_cum[zq : zq + 1, :], (128, 256)).T
        tops = []
        for half in range(2):
            lines = slice(half * 128, (half + 1) * 128)
            top = jnp.full((128, 128), NEG, F32)
            for zk in range(zq + 1):
                for i in range(n):
                    b = begin[zq] + zk * n + i
                    bias = (bias_edge if zk == zq else bias_full)[i][zk : zk + 1, :]
                    got = (
                        lax.dot_general(
                            queries[lines],
                            kvs[i][zk * 256 : (zk + 1) * 256, 0:128],
                            (((1,), (1,)), ((), ())),
                            preferred_element_type=F32,
                        )
                        * (scale * LOG2E)
                        - bias
                    )
                    if zk == zq and slots[i] == (True, 0):
                        got = jnp.where(causal[lines], got, NEG)
                    scores[lines, b * 256 : (b + 1) * 256] = got
                    top = jnp.maximum(top, jnp.maximum(got[:, 0:128], got[:, 128:256]))
            tops.append(top)
        top = jnp.concatenate(tops, axis=0)
        peak = jnp.broadcast_to(jnp.max(top, axis=1, keepdims=True), (256, 128)) + cum_t
        if not first:
            old = m_in[rows, :]
            peak = jnp.maximum(peak, old)
            keep[zq] = jnp.exp2(old - peak)
        shifts[zq] = cum_t - peak
        if not last:
            m_out[rows, :] = peak

    def weigh(zq):
        shift = jnp.concatenate([shifts[zq], shifts[zq]], axis=1)
        for b in range(begin[zq], begin[zq] + (zq + 1) * n):
            block = slice(b * 256, (b + 1) * 256)
            probs[:, block] = jnp.exp2(scores[:, block] + shift).astype(BF)

    def gather(zq):
        rows = slice(zq * 256, (zq + 1) * 256)
        blocks = (zq + 1) * n
        half = (blocks + 1) // 2
        acc = None
        for lo, hi in ((0, half), (half, blocks)):
            if lo == hi:
                continue
            part = jnp.dot(
                probs[:, (begin[zq] + lo) * 256 : (begin[zq] + hi) * 256],
                v_all[lo * 256 : hi * 256, :],
                preferred_element_type=F32,
            )
            acc = part if acc is None else acc + part
        if not first:
            acc = acc + acc_in[rows, :] * jnp.concatenate([keep[zq], keep[zq]], axis=1)
        if last:
            whole[rows, :] = (acc[:, 0:128] / acc[:, 128:256]).astype(BF)
        else:
            acc_out[rows, :] = acc

    for step in STEPS:
        {"s": score, "w": weigh, "g": gather}[step[0]](int(step[1]))
    if last:
        for s in range(4):
            zs = lax.rem(at[0] + s, 4)
            chunks[s][...] = whole[pl.ds(pl.multiple_of(zs * 256, 256), 256), :]


def emit_body(at, *refs):
    att, weights = refs[0:4], refs[4]
    outs = refs[5:9]
    joined, whole = refs[9:]
    z, x = at[0], at[3]
    for s in range(4):
        zs = slot_of(z, s, 4)
        joined[:, pl.ds(pl.multiple_of(zs * 128, 128), 128)] = att[s][...]
    whole[...] = lax.dot_general(
        joined[...], weights[...], (((1,), (1,)), ((), ())), preferred_element_type=F32
    )
    for s in range(4):
        xs = lax.rem(x + s, 4)
        got = whole[pl.ds(pl.multiple_of(xs * 64, 64), 64), :]
        outs[s][...] = got.astype(outs[s].dtype)


def finish_body(at, own, r1, r2, r3, gain, out):
    total = own[...] + r1[...].astype(F32) + r2[...].astype(F32) + r3[...].astype(F32)
    mean = jnp.mean(total * total, axis=1, keepdims=True)
    out[...] = (total * lax.rsqrt(mean + 1e-06) * gain[...]).astype(BF)


def shape(*dims, dtype=BF):
    return jax.ShapeDtypeStruct(dims, dtype)


TURN = (2, 1, 3)


def ring(axis, values):
    got = [values[0], None, None, None]
    for s in TURN:
        got[s] = around(axis, s, values[s], 4)
    return got


CUM_AT = {
    (True, 0): (0, 0),
    (False, 0): (1, 0),
    (True, 1): (2, 0),
    (False, 2): (2, 32),
    (False, 1): (3, 0),
    (True, 2): (3, 32),
    (True, 3): (4, 0),
    (False, 3): (4, 32),
}
STEPS = ("s2", "s3", "w2", "g2", "w3", "s1", "g3", "s0", "w1", "g1", "w0", "g0")
GROUPS = (
    ((True, 0), (False, 0)),
    ((True, 2),),
    ((False, 2), (True, 1)),
    ((False, 1), (True, 3)),
    ((False, 3),),
)


def layer(tokens, wq, wk, wv, gate, forget_bias, out_weight, out_gain):
    seq_len = tokens.shape[0] * 128

    *first, a_own = named(pack_body, [shape(128, 512)] * 4 + [shape(64, 512)], first=True)(
        tokens, wq, wk, wv, gate.T, out_weight.T
    )
    a_x = spread("x", a_own)
    by_z = ring("z", first)

    mine = jnp.concatenate([m[64:128] for m in by_z], axis=0)
    own_w = spread("y", mine)
    b_half = spread("x", jnp.concatenate([m[0:64] for m in by_z], axis=0))
    a_half = spread("z", jnp.concatenate(a_x, axis=0))
    other_w = [around("c", 1, w, 2) for w in own_w]

    early = named(stack_body, [shape(1024, 1024), shape(1024, 512)])(
        *a_half[:3], *b_half[:3], *own_w[:3], *other_w[:3]
    )
    kv, toks, weights = named(
        project_body,
        [shape(1024, 256), shape(1024, 1024), shape(1024, 512)],
        alias={4: 1, 5: 2},
    )(a_half[3], b_half[3], own_w[3], other_w[3], *early)
    q, cum = named(
        functools.partial(query_body, seq_len),
        [shape(1024, 128), shape(32, 256)],
        [pltpu.VMEM((8, 256), F32)],
    )(forget_bias.reshape(1, 4), toks, weights)

    cum_mate = around("c", 1, cum, 2)
    cum_pair = jnp.concatenate([cum, cum_mate], axis=0)
    cum_near = along("y", 1, cum_pair)
    cum_far = around("y", 2, cum_pair, 4)
    cums = [cum, cum_mate, cum_near, around("c", 1, cum_near, 2), cum_far]
    kv_own = spread("y", kv, step=-1)
    where = {(True, j): kv_own[j] for j in range(4)}
    where |= {(False, j): around("c", 1, kv_own[j], 2) for j in range(4)}

    state = ()
    for g, slots in enumerate(GROUPS):
        n = len(slots)
        first_call, last_call = g == 0, g == len(GROUPS) - 1
        outs = (
            [shape(256, 128)] * 4
            if last_call
            else [shape(1024, 128, dtype=F32), shape(1024, 256, dtype=F32)]
        )
        state = named(
            functools.partial(attend_body, slots, first_call, last_call, 128 ** -0.5),
            outs,
            [
                pltpu.VMEM((n * 1024, 256), BF),
                pltpu.VMEM((256, n * 2560), F32),
                pltpu.VMEM((256, n * 2560), BF),
                pltpu.VMEM((1024, 128), BF),
            ],
        )(q, *cums, *[where[s] for s in slots], *state)

    att = ring("z", state)
    laid = named(lay_body, [shape(1024, 512)])(*own_w, *other_w)
    own, *rest = named(
        emit_body,
        [shape(64, 1024, dtype=F32)] + [shape(64, 1024)] * 3,
        [
            pltpu.VMEM((256, 512), BF),
            pltpu.VMEM((256, 1024), F32),
        ],
    )(*att, *laid)
    got = ring("x", [own, *rest])
    (out,) = named(finish_body, [shape(64, 1024)], last=True)(
        *got, out_gain.reshape(1, 1024)
    )
    return out


def solution(mesh):
    torus = Mesh(mesh.devices.reshape(4, 4, 2, 4), ("z", "y", "c", "x"))
    sp = ("z", "y", "c")
    in_specs = (
        P(sp + ("x",), None),
        P(sp, "x"),
        P(sp, "x"),
        P(sp, "x"),
        P(sp, "x"),
        P("x"),
        P("x", sp),
        P(),
    )
    return jax.shard_map(
        layer, mesh=torus, in_specs=in_specs, out_specs=P(sp + ("x",), None), check_vma=False
    )
```
